256 devices in a mesh: sp: 16 (over y, x), tp: 16 (over z, core).
Axes of the slice: x: 4, y: 4, z: 8, core: 2. Of those that a mesh axis runs over, the one named last changes fastest.
Arguments:
- out_gate: bfloat16 [8192, 2048], P('sp', 'tp'), may hold values from -6 to 6
- in_gate: bfloat16 [8192, 2048], P('sp', 'tp'), may hold values from -6 to 6
- conv_input: bfloat16 [8192, 2048], P('sp', 'tp'), may hold values from -6 to 6
- conv_taps: bfloat16 [3, 2048], P(None, 'tp'), may hold values from -3.5 to 3.5
- documents: int32 [8192], P('sp'), may hold values from 0 to 8, never falling along the last dimension, each value on 1 to 1536 neighbouring positions
- out_weight: bfloat16 [2048, 2048], P('tp'), may hold values from -0.125 to 0.125
- residual: bfloat16 [8192, 2048], P(('sp', 'tp')), may hold values from -6 to 6
- norm_gain: bfloat16 [2048], replicated, may hold values from 0.099609375 to 1.8984375
- expert_ids: int32 [8192, 2], P(('sp', 'tp')), may hold values from 0 to 15, all different within a row; in each aligned block of 32 rows (0 to 31, 32 to 63, ...) at most 6 rows name the same one
- route_weights: float32 [8192, 2], P(('sp', 'tp')), may hold values from 0.1 to 1
- gate_weight: bfloat16 [16, 2048, 4096], P('sp', None, 'tp'), may hold values from -0.125 to 0.125
- up_weight: bfloat16 [16, 2048, 4096], P('sp', None, 'tp'), may hold values from -0.125 to 0.125
- down_weight: bfloat16 [16, 4096, 2048], P('sp', 'tp'), may hold values from -0.09375 to 0.09375
Outputs:
- layer_out: bfloat16 [8192, 2048], P(('sp', 'tp'))
The draws below stay inside these ranges and needn't reach their ends.
Inputs may be any that keep to these rules, and one draw needn't show every extreme that they name: `expert_ids`: A token's two experts differ; in each aligned block of 32 rows no expert is named by more than 6 entries, a bound that some block reaches. `documents`: document numbers never fall along the sequence; a document holds at most 1536 positions.
All inputs are finite; a program needn't handle non-finite values.
Results may differ from the reference program's by a relative error of at most 0.017.
Values may be sent and summed in bfloat16 or wider, within the bound.
A program may use at most 64 MiB of HBM per device.

```python
import math
import jax
import jax.numpy as jnp
import numpy as np
from jax import lax

D = 2048
F = 4096
TAPS = 3
TOK_DEV = 512
TOKENS = 8192
EXPERTS = 16
ROWS = 32
CAP = 6
N_SP = 16
N_TP = 16


def steps_of(own_key, extent, split, low, top_value):
    level = 1.0
    for axis_at, blocks in split:
        draws = jax.random.uniform(jax.random.fold_in(jax.random.fold_in(own_key, 6), axis_at), (blocks,), jnp.float32, low / len(split), top_value / len(split))
        level = level * jnp.repeat(jnp.exp(draws), extent[axis_at] // blocks).reshape((-1,) + (1,) * (len(extent) - 1 - axis_at))
    return level


def profile(number_of, total, bound, skew):
    loads = [(1 << 20) // math.isqrt(rank ** skew) + 1 for rank in range(2, number_of + 1)]
    rest, counts = total - bound - (number_of - 1), [1] * (number_of - 1)
    while rest > 0:
        free = [i for i in range(number_of - 1) if counts[i] < bound]
        pool, left = sum([loads[i] for i in free]), rest
        for i in free:
            extra = min(bound - counts[i], max(1, left * loads[i] // pool), rest)
            counts[i] = counts[i] + extra
            rest = rest - extra
    return np.array([bound] + counts)


def uneven(stream_key, number_of, total, most, lean):
    if number_of == 2:
        one = jax.random.randint(stream_key, (), max(1, total - most), min(most, total - 1) + 1)
        return jnp.stack([one, total - one])
    sizes = jnp.asarray(profile(number_of, total, most, lean), jnp.int32)
    couples = (number_of - 1) // 2
    source_of, taker = sizes[1:1 + 2 * couples:2], sizes[2:2 + 2 * couples:2]
    margin = jnp.minimum(source_of - 1, most - taker)
    shifted = jax.random.randint(jax.random.fold_in(stream_key, 1), (couples,), 0, 1 << 20) % (margin + 1)
    sizes = sizes.at[1:1 + 2 * couples:2].set(source_of - shifted).at[2:2 + 2 * couples:2].set(taker + shifted)
    return sizes[jax.random.permutation(jax.random.fold_in(stream_key, 2), number_of)]


def shared_out(key, own, number, rows, count, top, bound, lean):
    ranking = jax.random.permutation(key, count)
    packed, usual = shares(count, rows * top, bound, lean, True), shares(count, rows * top, bound, lean, False)
    places = jnp.arange(count)

    def named(tallies, rotation):
        used = int((tallies > 0).sum())
        fixed = max(1, used // 4)
        passed = fixed + (places - fixed + rotation * (used - fixed)) % max(1, count - fixed)
        return jnp.zeros((count,), jnp.int32).at[ranking[jnp.where(places < fixed, places, passed)]].set(jnp.asarray(tallies, jnp.int32))

    tallies = jnp.where(number % 4 == 0, named(packed, number // 4), named(usual, number - number // 4 - 1))
    mixed = jax.random.permutation(jax.random.fold_in(own, 3), count)
    source_of, taker = mixed[0:count // 2 * 2:2], mixed[1:count // 2 * 2:2]
    slack = jnp.minimum(tallies[source_of] - 1, bound - tallies[taker]) // 2
    slack = jnp.where((source_of == ranking[0]) | (taker == ranking[0]) | (tallies[taker] == 0), 0, jnp.maximum(slack, 0))
    passed = jax.random.randint(jax.random.fold_in(own, 4), (count // 2,), 0, 1 << 20) % (slack + 1)
    tallies = tallies.at[source_of].add(-passed).at[taker].add(passed)
    labels = jnp.searchsorted(jnp.cumsum(tallies), jnp.arange(rows * top), side="right").astype(jnp.int32)
    table = labels.reshape(top, rows).T
    table = table[jax.random.permutation(jax.random.fold_in(own, 1), rows)]
    rotation = jax.random.randint(jax.random.fold_in(own, 2), (rows, 1), 0, top)
    return jnp.take_along_axis(table, (jnp.arange(top)[None, :] + rotation) % top, axis=1)


def shares(number_of, total, limit, lean, full):
    weights = [(1 << 20) // math.isqrt(grade ** lean) + 1 for grade in range(1, number_of + 1)]
    largest = limit if full else min(limit, max(-(-total // number_of), total * weights[0] // sum(weights)))
    least = 1 if total - largest >= number_of - 1 else 0
    counts, spare = [largest] + [least] * (number_of - 1), total - largest - least * (number_of - 1)
    while spare > 0:
        free = [i for i in range(1, number_of) if counts[i] < largest] or [i for i in range(1, number_of) if counts[i] < limit]
        whole, budget = sum([weights[i] for i in free]), spare
        for i in free:
            addition = min(limit - counts[i], max(1, budget * weights[i] // whole), spare)
            counts[i] = counts[i] + addition
            spare = spare - addition
    return np.array(counts)


def noise(key, shape, deviation, most, pieces=(), kind=jnp.bfloat16):
    gain = steps_of(key, shape, pieces, -0.22, 0.18) if pieces else 1.0
    array = jax.random.normal(key, shape, jnp.float32) * deviation * gain
    return jnp.minimum(jnp.maximum(array, -most), most).astype(kind)


def setup_inputs(seed: int = 0) -> dict:
    streams_of = jax.random.split(jax.random.key(seed), 14)
    out_gate = noise(streams_of[0], (TOKENS, D), 1.0, 6.0, ((0, 16), (1, 16)))
    in_gate = noise(streams_of[1], (TOKENS, D), 1.0, 6.0, ((0, 16), (1, 16)))
    conv_input = noise(streams_of[2], (TOKENS, D), 1.0, 6.0, ((0, 16), (1, 16)))
    conv_taps = noise(streams_of[3], (TAPS, D), TAPS ** -0.5, 3.5, ((1, 16),))
    documents = jnp.searchsorted(jnp.cumsum(uneven(streams_of[4], N_SP // 2 + 1, TOKENS, 3 * TOK_DEV, 0)), jnp.arange(TOKENS), side="right").astype(jnp.int32)
    out_weight = noise(streams_of[5], (D, D), D ** -0.5, 0.125, ((0, 16),))
    residual = noise(streams_of[6], (TOKENS, D), 1.0, 6.0, ((0, 256),))
    norm_gain = jnp.clip(1.0 + 0.18 * jax.random.normal(streams_of[7], (D,), jnp.float32), 0.099609375, 1.8984375).astype(jnp.bfloat16)
    expert_ids_keys = jax.random.split(jax.random.fold_in(streams_of[8], 1), TOKENS // ROWS)
    expert_ids_turns = jax.random.permutation(jax.random.fold_in(streams_of[8], 3), TOKENS // ROWS)
    expert_ids = jax.vmap(lambda own, number: shared_out(jax.random.fold_in(streams_of[8], 2), own, number, ROWS, EXPERTS, 2, CAP, 2))(expert_ids_keys, expert_ids_turns).reshape((TOKENS, 2))
    route_weights = jnp.clip(0.1 + 0.9 * jax.random.uniform(streams_of[9], (TOKENS, 2), jnp.float32) ** steps_of(streams_of[9], (TOKENS, 2), ((0, 256),), -0.2, 0.2), 0.1, 1.0)
    gate_weight = noise(streams_of[10], (EXPERTS, D, F), D ** -0.5, 0.125, ((0, 16), (2, 16)))
    up_weight = noise(streams_of[11], (EXPERTS, D, F), D ** -0.5, 0.125, ((0, 16), (2, 16)))
    down_weight = noise(streams_of[12], (EXPERTS, F, D), F ** -0.5, 0.09375, ((0, 16), (1, 16)))
    return dict(out_gate=out_gate, in_gate=in_gate, conv_input=conv_input, conv_taps=conv_taps, documents=documents, out_weight=out_weight, residual=residual, norm_gain=norm_gain, expert_ids=expert_ids, route_weights=route_weights, gate_weight=gate_weight, up_weight=up_weight, down_weight=down_weight)


EPS = 1e-06

def slot_index(expert_ids, experts, capacity):
    listed = expert_ids.reshape(-1).astype(jnp.int32)
    onehot = (listed[:, None] == jnp.arange(experts, dtype=jnp.int32)[None, :]).astype(jnp.int32)
    earlier = (jnp.cumsum(onehot, axis=0) - onehot).astype(jnp.int32)
    within = lax.optimization_barrier(jnp.sum(earlier * onehot, axis=1)).astype(jnp.int32)
    return (listed * capacity + within).astype(jnp.int32)

def dispatch_block(target, block_rows):
    count = block_rows.shape[0]
    slots = jnp.arange(EXPERTS * CAP, dtype=jnp.int32)
    table = lax.optimization_barrier(jnp.sum((target.reshape(count, 2)[:, :, None] == slots[None, None, :]).astype(jnp.float32), axis=1))
    placed = lax.dot_general(table, block_rows.astype(jnp.float32), (((0,), (0,)), ((), ())))
    return placed.astype(jnp.bfloat16)

def run_expert(operands):
    expert_in, gate_part, up_part, down_part = operands
    gate_proj = jnp.dot(expert_in, gate_part, preferred_element_type=jnp.float32)
    up_proj = jnp.dot(expert_in, up_part, preferred_element_type=jnp.float32)
    act = (jax.nn.silu(gate_proj) * up_proj).astype(jnp.bfloat16)
    width = F // N_TP

    def add_block(total, index):
        columns = lax.dynamic_slice_in_dim(act, index * width, width, 1)
        weight_rows = lax.dynamic_slice_in_dim(down_part, index * width, width, 0)
        partial_sum = lax.optimization_barrier(jnp.dot(columns, weight_rows, preferred_element_type=jnp.float32).astype(jnp.bfloat16))
        return (total + partial_sum.astype(jnp.float32), None)
    total, ignored = lax.scan(add_block, jnp.zeros((expert_in.shape[0], D), jnp.float32), jnp.arange(N_TP, dtype=jnp.int32))
    return total.astype(jnp.bfloat16)

def reference(out_gate, in_gate, conv_input, conv_taps, documents, out_weight, residual, norm_gain, expert_ids, route_weights, gate_weight, up_weight, down_weight):
    length = conv_input.shape[0]
    signal = in_gate.astype(jnp.float32) * conv_input.astype(jnp.float32)
    tap_values = conv_taps.astype(jnp.float32)
    position = jnp.arange(length, dtype=jnp.int32)
    mixed_conv = tap_values[2][None, :] * signal
    for offset in (1, 2):
        earlier_signal = jnp.pad(signal, ((offset, 0), (0, 0)))[:length]
        earlier_docs = jnp.pad(documents, (offset, 0))[:length]
        allowed = (position >= offset) & (earlier_docs == documents)
        mixed_conv = mixed_conv + jnp.where(allowed[:, None], tap_values[2 - offset][None, :] * earlier_signal, 0.0)
    gated = (out_gate.astype(jnp.float32) * mixed_conv).astype(jnp.bfloat16)
    width = D // N_TP

    def add_block(total, index):
        columns = lax.dynamic_slice_in_dim(gated, index * width, width, 1)
        weight_rows = lax.dynamic_slice_in_dim(out_weight, index * width, width, 0)
        partial_sum = lax.optimization_barrier(jnp.dot(columns, weight_rows, preferred_element_type=jnp.float32).astype(jnp.bfloat16))
        return (total + partial_sum.astype(jnp.float32), None)
    mixed, ignored = lax.scan(add_block, jnp.zeros((length, D), jnp.float32), jnp.arange(N_TP, dtype=jnp.int32))
    hidden_state = (residual.astype(jnp.float32) + mixed).astype(jnp.bfloat16)
    hidden_wide = hidden_state.astype(jnp.float32)
    stats = lax.optimization_barrier(jnp.mean(hidden_wide * hidden_wide, axis=-1, keepdims=True))
    normed = (hidden_wide * lax.rsqrt(stats + EPS) * norm_gain.astype(jnp.float32)[None, :]).astype(jnp.bfloat16)
    block_count = N_SP * N_TP
    normed_blocks = normed.reshape(block_count, ROWS, D)
    route_blocks = expert_ids.reshape(block_count, ROWS, 2)
    targets = jax.vmap(lambda ids: slot_index(ids, EXPERTS, CAP))(route_blocks)
    buffers = jax.vmap(dispatch_block)(targets, normed_blocks)
    expert_rows = buffers.reshape(block_count, EXPERTS, CAP, D).transpose(1, 0, 2, 3).reshape(EXPERTS, block_count * CAP, D)
    expert_out = lax.map(run_expert, (expert_rows, gate_weight, up_weight, down_weight))
    returned = expert_out.reshape(EXPERTS, block_count, CAP, D).transpose(1, 0, 2, 3).reshape(block_count, EXPERTS * CAP, D)
    picked = jax.vmap(lambda table, target: table[target])(returned, targets)
    picked = picked.astype(jnp.float32).reshape(block_count, ROWS, 2, D)
    weights = route_weights.astype(jnp.float32).reshape(block_count, ROWS, 2)
    combined = lax.optimization_barrier(jnp.sum(picked * weights[:, :, :, None], axis=2)).reshape(length, D)
    return (hidden_wide + combined).astype(jnp.bfloat16)
```

```python
import jax
import jax.numpy as jnp
from jax import lax
from jax.experimental import pallas as pl
from jax.experimental.pallas import tpu as pltpu
from jax.sharding import PartitionSpec as P

EPS = 1e-06
MESH = pl.DeviceIdType.MESH
F32 = jnp.float32
BF16 = jnp.bfloat16

GATHER = {0: ((0, 1, 2, 3), (0, 7, 6)), 1: ((0, 1, 2), (0, 7, 6, 5))}
REDUCE = {0: ((4, 5, 6, 7), (3, 2, 1)), 1: ((5, 6, 7), (4, 3, 2, 1))}


def dot(a, b):
    return jnp.dot(a, b, preferred_element_type=F32)


def dot_t(a, b):
    return lax.dot_general(a, b, (((0,), (0,)), ((), ())), preferred_element_type=F32)


def kernel(
    og_ref, ig_ref, ci_ref, taps_ref, docs_ref, ow_ref, res_ref, gain_ref, ids_ref, rw_ref, gw_ref, uw_ref, dw_ref,
    out_ref,
    h_ig, h_ci, h_docs, ext, extd, gbuf, xa, wa, part1, rbuf1, hid, nrm,
    tmain, ttail, sel, outg, xbuf, x2, act, wg, wu, wd, part, rbuf, ret,
    loc_sem, halo_s, halo_r, duo_s, duo_r, rs1_s, rs1_r, disp_s, disp_r, ag_s, ag_r, rs_s, rs_r, ret_s, ret_r,
):
    sp = lax.axis_index("sp")
    tp = lax.axis_index("tp")
    n_sp = lax.axis_size("sp")
    core = lax.rem(tp, 2)
    z = tp // 2
    right = {"tp": lax.rem(z + 1, 8) * 2 + core}
    left = {"tp": lax.rem(z + 7, 8) * 2 + core}
    partner = {"tp": z * 2 + 1 - core}

    def sp_at(d):
        return {"sp": lax.rem(sp + d, n_sp)}

    def remote(src, dst, ssem, rsem, device):
        return pltpu.make_async_remote_copy(
            src_ref=src, dst_ref=dst, send_sem=ssem, recv_sem=rsem, device_id=device, device_id_type=MESH
        )

    local = [
        pltpu.make_async_copy(ow_ref, wa.at[0], loc_sem.at[0]),
        pltpu.make_async_copy(gw_ref.at[0], wg.at[0], loc_sem.at[1]),
        pltpu.make_async_copy(uw_ref.at[0], wu.at[0], loc_sem.at[2]),
        pltpu.make_async_copy(dw_ref.at[0], wd.at[0], loc_sem.at[3]),
    ]
    for c in local:
        c.start()

    barrier = pltpu.get_barrier_semaphore()
    for device in [right, left, partner]:
        pl.semaphore_signal(barrier, inc=1, device_id=device, device_id_type=MESH)
    for d in range(1, 16):
        pl.semaphore_signal(barrier, inc=1, device_id=sp_at(d), device_id_type=MESH)
    pl.semaphore_wait(barrier, 18)

    halo = [
        remote(ig_ref.at[pl.ds(496, 16)], h_ig, halo_s.at[0], halo_r.at[0], sp_at(1)),
        remote(ci_ref.at[pl.ds(496, 16)], h_ci, halo_s.at[1], halo_r.at[1], sp_at(1)),
        remote(docs_ref, h_docs, halo_s.at[2], halo_r.at[2], sp_at(1)),
    ]
    for c in halo:
        c.start()
    w_duo = remote(ow_ref, wa.at[1], duo_s.at[0], duo_r.at[0], partner)
    w_duo.start()

    rows = lax.broadcasted_iota(jnp.int32, (128, 32), 0)
    rel, sub = rows // 8, lax.rem(rows, 8)
    rid = lax.rem(ids_ref[...] - sp + 16, 16)
    one = [(jnp.broadcast_to(rid[k : k + 1, :], (128, 32)) == rel) for k in range(2)]
    both = (one[0] | one[1]).astype(F32)
    before = (
        lax.broadcasted_iota(jnp.int32, (32, 32), 0) < lax.broadcasted_iota(jnp.int32, (32, 32), 1)
    ).astype(BF16)
    place = dot(both.astype(BF16), before)
    hit = [jnp.where(place == sub.astype(F32), 1.0, 0.0)]
    for j in range(3):
        hit.append(
            jnp.where(((sub == 6) & (place == float(j))) | ((sub == 7) & (place == j + 3.0)), 1.0, 0.0)
        )
    hit[0] = jnp.where(sub < 6, hit[0], 0.0)
    tmain[...] = (hit[0] * both).astype(BF16)
    for j in range(3):
        ttail[j] = (hit[1 + j] * both).astype(BF16)
    sr = lax.broadcasted_iota(jnp.int32, (128, 128), 0)
    sc = lax.broadcasted_iota(jnp.int32, (128, 128), 1)
    same = (sr // 8) == (sc // 8)
    rr, rc = lax.rem(sr, 8), lax.rem(sc, 8)
    for j in range(3):
        sel[j] = jnp.where(
            same & (((rr == j) & (rc == 6)) | ((rr == j + 3) & (rc == 7))), 1.0, 0.0
        ).astype(BF16)
        sel[3 + j] = jnp.where(
            same & (((rc == j) & (rr == 6)) | ((rc == j + 3) & (rr == 7))), 1.0, 0.0
        ).astype(BF16)

    sig = ig_ref[...].astype(F32) * ci_ref[...].astype(F32)
    ext[pl.ds(16, 512), :] = sig
    docs = docs_ref[...].astype(F32)
    for i in range(4):
        extd[pl.ds(16 + 128 * i, 128), :] = jnp.broadcast_to(docs[i : i + 1, :], (128, 128)).T
    for c in halo:
        c.wait_recv()
    ext[pl.ds(0, 16), :] = h_ig[...].astype(F32) * h_ci[...].astype(F32)
    old = jnp.broadcast_to(h_docs[...].astype(F32)[3:4, :], (128, 128)).T
    extd[pl.ds(0, 16), :] = old[112:128, :]
    taps = taps_ref[...].astype(F32)
    pos = sp * 512 + lax.broadcasted_iota(jnp.int32, (512, 128), 0)
    now = extd[pl.ds(16, 512), :]
    conv = taps[2:3, :] * sig
    for off in (1, 2):
        ok = (pos >= off) & (extd[pl.ds(16 - off, 512), :] == now)
        conv = conv + jnp.where(ok, taps[2 - off : 3 - off, :] * ext[pl.ds(16 - off, 512), :], 0.0)
    gated = (og_ref[...].astype(F32) * conv).astype(BF16)
    for j in range(16):
        gbuf[j % 2, pl.ds(32 * (j // 2), 32), :] = gated[32 * j : 32 * j + 32, :]
    g_duo = remote(gbuf.at[1 - core], gbuf.at[2], duo_s.at[1], duo_r.at[1], partner)
    g_duo.start()
    xa[:, pl.ds(0, 128)] = gbuf[core]

    local[0].wait()
    w_duo.wait_recv()
    g_duo.wait_recv()
    xa[:, pl.ds(128, 128)] = gbuf[2]
    for p in range(4):
        cols = pl.ds(512 * p, 512)
        prod = dot(xa[:, pl.ds(0, 128)], wa[0, :, cols]) + dot(xa[:, pl.ds(128, 128)], wa[1, :, cols])
        part1[p] = prod.astype(BF16).reshape(8, 32, 512)
    e_duo = [
        remote(gw_ref.at[0], wg.at[1], duo_s.at[2], duo_r.at[2], partner),
        remote(uw_ref.at[0], wu.at[1], duo_s.at[3], duo_r.at[3], partner),
        remote(dw_ref.at[0], wd.at[1], duo_s.at[4], duo_r.at[4], partner),
    ]
    for c in e_duo:
        c.start()

    pending = [w_duo, g_duo] + halo + e_duo

    def reduce_hop(piece, way, hop, part_at, rbuf_at, ssem, rsem):
        slots = REDUCE[piece % 2][way]
        here = part_at(piece, slots[hop])
        if hop > 0:
            c = remote(here, rbuf_at(piece, way, hop - 1), ssem.at[piece, way, hop - 1], rsem.at[piece, way, hop - 1],
                       (right, left)[way])
            c.wait_recv()
            here[...] = (here[...].astype(F32) + rbuf_at(piece, way, hop - 1)[...].astype(F32)).astype(BF16)
        c = remote(here, rbuf_at(piece, way, hop), ssem.at[piece, way, hop], rsem.at[piece, way, hop],
                   (right, left)[way])
        c.start()
        pending.append(c)

    def reduce_tick(t, pieces, *rest):
        for piece in pieces:
            for way in range(2):
                hop = t - (4 - len(REDUCE[piece % 2][way]))
                if hop >= 0:
                    reduce_hop(piece, way, hop, *rest)

    def reduce_last(piece, part_at, rbuf_at, ssem, rsem):
        total = part_at(piece, 0)[...].astype(F32)
        for way in range(2):
            hop = len(REDUCE[piece % 2][way]) - 1
            here = rbuf_at(piece, way, hop)
            remote(here, here, ssem.at[piece, way, hop], rsem.at[piece, way, hop], (right, left)[way]).wait_recv()
            total = total + here[...].astype(F32)
        return total

    args1 = (
        lambda p, s: part1.at[p, lax.rem(z - s + 8, 8)],
        lambda p, w, h: rbuf1.at[p, w, h],
        rs1_s,
        rs1_r,
    )
    for t in range(4):
        reduce_tick(t, range(4), *args1)
    square = jnp.zeros((32, 1), F32)
    for p in range(4):
        cols = pl.ds(512 * p, 512)
        wide = (res_ref[:, cols].astype(F32) + reduce_last(p, *args1)).astype(BF16)
        hid[:, cols] = wide
        wide = wide.astype(F32)
        square = square + jnp.sum(wide * wide, axis=1, keepdims=True)
    scale = lax.rsqrt(square * (1.0 / 2048.0) + EPS)
    for p in range(4):
        cols = pl.ds(512 * p, 512)
        nrm[:, cols] = (hid[:, cols].astype(F32) * scale * gain_ref[:, cols].astype(F32)).astype(BF16)

    tail = nrm[:, pl.ds(1536, 512)]
    for j in range(3):
        cols = pl.ds(512 * j, 512)
        packed = (dot(tmain[...], nrm[:, cols]) + dot(ttail[j], tail)).astype(BF16)
        outg[:, :, cols] = packed.reshape(16, 8, 512)
    disp = {}
    for d in range(1, 16):
        disp[d] = remote(outg.at[d], xbuf.at[0, d], disp_s.at[d], disp_r.at[d], sp_at(d))
        disp[d].start()
    xbuf[0, 0] = outg[0]

    def piece_at(buf, slot, piece):
        return buf.at[slot, pl.ds(4 * piece, 4)]

    def gather_hop(piece, way, hop):
        slot = GATHER[piece % 2][way][hop]
        to = (slot + 1) % 8 if way == 0 else (slot + 7) % 8
        c = remote(piece_at(xbuf, slot, piece), piece_at(xbuf, to, piece), ag_s.at[piece, to], ag_r.at[piece, to],
                   (right, left)[way])
        c.start()
        pending.append(c)

    def gather_wait(piece, slot):
        here = piece_at(xbuf, slot, piece)
        remote(here, here, ag_s.at[piece, slot], ag_r.at[piece, slot], right).wait_recv()

    def gather_start(pair):
        for piece in (2 * pair, 2 * pair + 1):
            for d in range(4 * piece, 4 * piece + 4):
                if d > 0:
                    disp[d].wait_recv()
            for way in range(2):
                gather_hop(piece, way, 0)

    def gather_tick(pair, k):
        for piece in (2 * pair, 2 * pair + 1):
            for way in range(2):
                slots = GATHER[piece % 2][way]
                if k <= len(slots):
                    gather_wait(piece, k if way == 0 else 8 - k)
                if k < len(slots):
                    gather_hop(piece, way, k)

    def expert(pair, slots):
        for i, slot in enumerate(slots):
            x2[pl.ds(64 * i, 64), pl.ds(0, 1536)] = xbuf[slot, pl.ds(8 * pair, 8)].reshape(64, 1536)
        tail = jnp.zeros((128, 512), F32)
        for j in range(3):
            tail = tail + dot(sel[j], x2[:, pl.ds(512 * j, 512)])
        x2[:, pl.ds(1536, 512)] = tail.astype(BF16)

        @pl.loop(0, 2)
        def _(h):
            gate = dot(x2[...], wg[h])
            up = dot(x2[...], wu[h])
            act[h] = (gate / (1.0 + jnp.exp(-gate)) * up).astype(BF16)

        def down(cols):
            return dot(act[0], wd[0, :, cols]) + dot(act[1], wd[1, :, cols])

        tail = down(pl.ds(1536, 512)).astype(BF16)
        low = lax.rem(lax.broadcasted_iota(jnp.int32, (128, 512), 0), 8) < 6

        @pl.loop(0, 3)
        def _(j):
            cols = pl.ds(pl.multiple_of(512 * j, 512), 512)
            packed = jnp.where(low, down(cols), dot(sel[3 + j], tail)).astype(BF16)
            for i, slot in enumerate(slots):
                part[slot, pl.ds(8 * pair, 8), :, cols] = packed[64 * i : 64 * i + 64].reshape(8, 8, 512)

    args = (
        lambda p, s: piece_at(part, s, p),
        lambda p, w, h: rbuf.at[p, w, h],
        rs_s,
        rs_r,
    )

    back = {}

    def send_back(pair):
        for piece in (2 * pair, 2 * pair + 1):
            total = reduce_last(piece, *args).astype(BF16)
            outg[pl.ds(4 * piece, 4)] = total
            for i in range(4):
                d = 4 * piece + i
                if d == 0:
                    ret[0] = total[0]
                else:
                    back[d] = remote(outg.at[d], ret.at[d], ret_s.at[d], ret_r.at[d], sp_at(16 - d))
                    back[d].start()
                    pending.append(back[d])

    gather_start(0)
    for c in local[1:]:
        c.wait()
    for c in e_duo:
        c.wait_recv()
    for k in (1, 2, 3):
        gather_tick(0, k)
        if k == 3:
            gather_start(1)
        expert(0, (k, 8 - k))
    gather_tick(0, 4)
    expert(0, (4, 0))
    for d in range(1, 16):
        disp[d].wait_send()
    for k in range(4):
        reduce_tick(k, (0, 1), *args)
        if k < 3:
            gather_tick(1, k + 1)
            expert(1, (k + 1, 7 - k))
        else:
            gather_tick(1, 4)
            expert(1, (4, 0))
    reduce_tick(0, (2, 3), *args)
    send_back(0)
    for k in range(1, 4):
        reduce_tick(k, (2, 3), *args)
    send_back(1)

    for d in range(1, 16):
        back[d].wait_recv()
    rw = rw_ref[...]
    weight = jnp.where(one[0], jnp.broadcast_to(rw[0:1, :], (128, 32)), 0.0) + jnp.where(
        one[1], jnp.broadcast_to(rw[1:2, :], (128, 32)), 0.0
    )
    parts = []
    for _ in range(3):
        parts.append(weight.astype(BF16))
        weight = weight - parts[-1].astype(F32)
    last = jnp.zeros((32, 512), F32)
    for j in range(3):
        cols = pl.ds(512 * j, 512)
        block = ret[:, :, cols].reshape(128, 512)
        acc = jnp.zeros((32, 512), F32)
        for w in parts:
            acc = acc + dot_t(w * tmain[...], block)
            last = last + dot_t(w * ttail[j], block)
        out_ref[:, cols] = (hid[:, cols].astype(F32) + acc).astype(BF16)
    cols = pl.ds(1536, 512)
    out_ref[:, cols] = (hid[:, cols].astype(F32) + last).astype(BF16)
    for c in pending:
        c.wait_send()


def shards(
    out_gate, in_gate, conv_input, conv_taps, documents, out_weight, residual, norm_gain, expert_ids, route_weights,
    gate_weight, up_weight, down_weight,
):
    vmem = pl.BlockSpec(memory_space=pltpu.VMEM)
    hbm = pl.BlockSpec(memory_space=pl.ANY)
    dma = pltpu.SemaphoreType.DMA
    scratch = [
        pltpu.VMEM((16, 128), BF16),
        pltpu.VMEM((16, 128), BF16),
        pltpu.VMEM((4, 128), jnp.int32),
        pltpu.VMEM((528, 128), F32),
        pltpu.VMEM((528, 128), F32),
        pltpu.VMEM((3, 256, 128), BF16),
        pltpu.VMEM((256, 256), BF16),
        pltpu.VMEM((2, 128, 2048), BF16),
        pltpu.VMEM((4, 8, 32, 512), BF16),
        pltpu.VMEM((4, 2, 4, 32, 512), BF16),
        pltpu.VMEM((32, 2048), BF16),
        pltpu.VMEM((32, 2048), BF16),
        pltpu.VMEM((128, 32), BF16),
        pltpu.VMEM((3, 128, 32), BF16),
        pltpu.VMEM((6, 128, 128), BF16),
        pltpu.VMEM((16, 8, 1536), BF16),
        pltpu.VMEM((8, 16, 8, 1536), BF16),
        pltpu.VMEM((128, 2048), BF16),
        pltpu.VMEM((2, 128, 256), BF16),
        pltpu.VMEM((2, 2048, 256), BF16),
        pltpu.VMEM((2, 2048, 256), BF16),
        pltpu.VMEM((2, 256, 2048), BF16),
        pltpu.VMEM((8, 16, 8, 1536), BF16),
        pltpu.VMEM((4, 2, 4, 4, 8, 1536), BF16),
        pltpu.VMEM((16, 8, 1536), BF16),
        dma((4,)),
        dma((3,)),
        dma((3,)),
        dma((5,)),
        dma((5,)),
        dma((4, 2, 4)),
        dma((4, 2, 4)),
        dma((16,)),
        dma((16,)),
        dma((4, 8)),
        dma((4, 8)),
        dma((4, 2, 4)),
        dma((4, 2, 4)),
        dma((16,)),
        dma((16,)),
    ]
    return pl.pallas_call(
        kernel,
        out_shape=jax.ShapeDtypeStruct((32, 2048), BF16),
        in_specs=[vmem] * 5 + [hbm] + [vmem] * 4 + [hbm] * 3,
        out_specs=vmem,
        scratch_shapes=scratch,
        compiler_params=pltpu.CompilerParams(
            collective_id=0, has_side_effects=True, vmem_limit_bytes=56 * 1024 * 1024
        ),
        name="layer",
    )(
        out_gate, in_gate, conv_input, conv_taps, documents.reshape(4, 128), out_weight, residual,
        norm_gain.reshape(1, 2048), expert_ids.T, route_weights.T, gate_weight, up_weight, down_weight,
    )


def solution(mesh):
    in_specs = (
        P("sp", "tp"),
        P("sp", "tp"),
        P("sp", "tp"),
        P(None, "tp"),
        P("sp"),
        P("tp", None),
        P(("sp", "tp"), None),
        P(),
        P(("sp", "tp"), None),
        P(("sp", "tp"), None),
        P("sp", None, "tp"),
        P("sp", None, "tp"),
        P("sp", "tp", None),
    )
    out_specs = P(("sp", "tp"), None)
    return jax.shard_map(shards, mesh=mesh, in_specs=in_specs, out_specs=out_specs, check_vma=False)
```

```python
import jax
import jax.numpy as jnp
from jax import lax
from jax.experimental import pallas as pl
from jax.experimental.pallas import tpu as pltpu
from jax.sharding import PartitionSpec as P

EPS = 1e-06
MESH = pl.DeviceIdType.MESH
F32 = jnp.float32
BF16 = jnp.bfloat16

GATHER = {0: ((0, 1, 2, 3), (0, 7, 6)), 1: ((0, 1, 2), (0, 7, 6, 5))}
REDUCE = {0: ((4, 5, 6, 7), (3, 2, 1)), 1: ((5, 6, 7), (4, 3, 2, 1))}
GROUPS = ((0, 1, 7, 2), (6, 3, 5, 4))
DY = (0, 2, 1, 3)
ORDER = (6, 5, 7, 4, 2, 1, 3, 10, 14, 9, 11, 13, 15, 8, 12)


def dot(a, b):
    return jnp.dot(a, b, preferred_element_type=F32)


def dot_t(a, b):
    return lax.dot_general(a, b, (((0,), (0,)), ((), ())), preferred_element_type=F32)


def iota(shape, dim):
    return lax.broadcasted_iota(jnp.int32, shape, dim)


def natural(q):
    d = (q * 2731) >> 16
    rest = q - 24 * d
    k = (rest * 10923) >> 16
    return d, k, rest - 6 * k


def kernel(
    og_hbm, ig_hbm, ci_hbm, taps_hbm, docs_hbm, ow_ref, res_hbm, gain_hbm, ids_hbm, rw_hbm, gw_ref, uw_ref, dw_ref,
    out_ref,
    og_ref, ig_ref, ci_ref, taps_ref, docs_ref, res_ref, gain_ref, ids_ref, rw_ref,
    h_ig, h_ci, h_docs, ext, extd, gbuf, xa, wa, part1, rbuf1, hid, nrm,
    line, meta, tmain, ttail, tdisp, tcomb, gm, gt, gmt, gtt,
    tok, outg, out2, xbuf, x2buf, xcat, x2, act, wg, wu, wd, part, rbuf, y2, back2, cpart, rbuf2, fin, ret,
    loc_sem, halo_s, halo_r, duo_s, duo_r, meta_s, meta_r, rs1_s, rs1_r, tok_s, tok_r, disp_s, disp_r, ag_s, ag_r,
    disp2_s, disp2_r, rs_s, rs_r, ret2_s, ret2_r, rs2_s, rs2_r, ret_s, ret_r,
):
    sp = lax.axis_index("sp")
    tp = lax.axis_index("tp")
    core = lax.rem(tp, 2)
    z = tp // 2
    y, x = sp // 4, lax.rem(sp, 4)
    right = {"tp": lax.rem(z + 1, 8) * 2 + core}
    left = {"tp": lax.rem(z + 7, 8) * 2 + core}
    sides = (right, left)
    partner = {"tp": z * 2 + 1 - core}
    following = {"sp": lax.rem(sp + 1, 16)}

    def ahead(d):
        return {"sp": lax.rem(y + DY[d // 4], 4) * 4 + lax.rem(x + d % 4, 4)}

    def behind(d):
        return {"sp": lax.rem(y + 4 - DY[d // 4], 4) * 4 + lax.rem(x + 4 - d % 4, 4)}

    def remote(src, dst, ssem, rsem, device):
        return pltpu.make_async_remote_copy(
            src_ref=src, dst_ref=dst, send_sem=ssem, recv_sem=rsem, device_id=device, device_id_type=MESH
        )

    pending = []

    def send(*args):
        c = remote(*args)
        c.start()
        pending.append(c)
        return c

    barrier = pltpu.get_barrier_semaphore()
    for device in [right, left, partner]:
        pl.semaphore_signal(barrier, inc=1, device_id=device, device_id_type=MESH)
    for d in range(1, 16):
        pl.semaphore_signal(barrier, inc=1, device_id=ahead(d), device_id_type=MESH)

    pairs = [
        (ids_hbm, ids_ref), (rw_hbm, rw_ref), (ig_hbm, ig_ref), (ci_hbm, ci_ref), (docs_hbm, docs_ref),
        (taps_hbm, taps_ref), (og_hbm, og_ref), (ow_ref, wa.at[0]), (res_hbm, res_ref), (gain_hbm, gain_ref),
        (gw_ref.at[0], wg.at[0]), (uw_ref.at[0], wu.at[0]), (dw_ref.at[0], wd.at[0]),
    ]
    local = [pltpu.make_async_copy(a, b, loc_sem.at[i]) for i, (a, b) in enumerate(pairs)]
    for c in local:
        c.start()

    local[0].wait()
    local[1].wait()
    ids = ids_ref[...]
    dy = ((ids >> 2) - y + 4) & 3
    rid = ((dy >> 1) + 2 * (dy & 1)) * 4 + (((ids & 3) - x + 4) & 3)
    weight = rw_ref[...]
    high = weight.astype(BF16).astype(F32)
    line[pl.ds(0, 2), :] = rid.astype(F32)
    line[pl.ds(2, 2), :] = high
    line[pl.ds(4, 2), :] = (weight - high).astype(BF16).astype(F32)
    line[pl.ds(6, 2), :] = jnp.zeros((2, 32), F32)
    spread = (iota((32, 128), 0) == (iota((32, 128), 1) & 31)).astype(BF16)
    meta[0] = dot(line[...].astype(BF16), spread)

    local[2].wait()
    local[3].wait()
    local[4].wait()
    local[5].wait()
    local[6].wait()
    ext[pl.ds(16, 512), :] = ig_ref[...].astype(F32) * ci_ref[...].astype(F32)
    docs = docs_ref[...].astype(F32)
    for i in range(4):
        extd[pl.ds(16 + 128 * i, 128), :] = jnp.broadcast_to(docs[i : i + 1, :], (128, 128)).T
    taps = taps_ref[...].astype(F32)

    def gated(first, count):
        pos = sp * 512 + first + iota((count, 128), 0)
        now = extd[pl.ds(16 + first, count), :]
        conv = taps[2:3, :] * ext[pl.ds(16 + first, count), :]
        for off in (1, 2):
            ok = (pos >= off) & (extd[pl.ds(16 + first - off, count), :] == now)
            earlier = taps[2 - off : 3 - off, :] * ext[pl.ds(16 + first - off, count), :]
            conv = conv + jnp.where(ok, earlier, 0.0)
        return (og_ref[pl.ds(first, count), :].astype(F32) * conv).astype(BF16)

    for j in range(1, 16):
        gbuf[j % 2, pl.ds(32 * (j // 2), 32), :] = gated(32 * j, 32)

    pl.semaphore_wait(barrier, 18)

    halo = [
        send(ig_hbm.at[pl.ds(496, 16)], h_ig, halo_s.at[0], halo_r.at[0], following),
        send(ci_hbm.at[pl.ds(496, 16)], h_ci, halo_s.at[1], halo_r.at[1], following),
        send(docs_hbm, h_docs, halo_s.at[2], halo_r.at[2], following),
    ]
    w_duo = send(ow_ref, wa.at[1], duo_s.at[0], duo_r.at[0], partner)

    def meta_tick(k):
        for way in range(2):
            slots = GATHER[0][way]
            if 0 < k <= len(slots):
                here = meta.at[k if way == 0 else 8 - k]
                sems = (meta_s.at[k if way == 0 else 8 - k], meta_r.at[k if way == 0 else 8 - k])
                remote(here, here, *sems, sides[way]).wait_recv()
            if k < len(slots):
                to = (slots[k] + 1) % 8 if way == 0 else (slots[k] + 7) % 8
                send(meta.at[slots[k]], meta.at[to], meta_s.at[to], meta_r.at[to], sides[way])

    meta_tick(0)
    for c in halo:
        c.wait_recv()
    ext[pl.ds(0, 16), :] = h_ig[...].astype(F32) * h_ci[...].astype(F32)
    old = jnp.broadcast_to(h_docs[...].astype(F32)[3:4, :], (128, 128)).T
    extd[pl.ds(0, 16), :] = old[112:128, :]
    gbuf[0, pl.ds(0, 32), :] = gated(0, 32)
    g_duo = send(gbuf.at[1 - core], gbuf.at[2], duo_s.at[1], duo_r.at[1], partner)
    xa[:, pl.ds(0, 128)] = gbuf[core]

    rows = iota((128, 32), 0)
    rel, sub = rows >> 3, (rows & 7).astype(F32)
    one = [(jnp.broadcast_to(rid[k : k + 1, :], (128, 32)) == rel) for k in range(2)]
    both = (one[0] | one[1]).astype(F32)
    before = (iota((32, 32), 0) < iota((32, 32), 1)).astype(BF16)
    place = dot(both.astype(BF16), before)
    tmain[...] = (jnp.where((place == sub) & (sub < 6.0), 1.0, 0.0) * both).astype(BF16)
    for j in range(3):
        hit = ((sub == 6.0) & (place == float(j))) | ((sub == 7.0) & (place == j + 3.0))
        ttail[j] = (jnp.where(hit, 1.0, 0.0) * both).astype(BF16)

    local[7].wait()
    w_duo.wait_recv()
    g_duo.wait_recv()
    xa[:, pl.ds(128, 128)] = gbuf[2]

    def reduce_hop(piece, way, hop, part_at, rbuf_at, ssem, rsem):
        slots = REDUCE[piece % 2][way]
        here = part_at(piece, slots[hop])
        if hop > 0:
            came = rbuf_at(piece, way, hop - 1)
            remote(came, came, ssem.at[piece, way, hop - 1], rsem.at[piece, way, hop - 1], sides[way]).wait_recv()
            here[...] = (here[...].astype(F32) + came[...].astype(F32)).astype(BF16)
        send(here, rbuf_at(piece, way, hop), ssem.at[piece, way, hop], rsem.at[piece, way, hop], sides[way])

    def reduce_tick(t, pieces, *rest):
        for piece in pieces:
            for way in range(2):
                hop = t - (4 - len(REDUCE[piece % 2][way]))
                if hop >= 0:
                    reduce_hop(piece, way, hop, *rest)

    def reduce_last(piece, part_at, rbuf_at, ssem, rsem):
        total = part_at(piece, 0)[...].astype(F32)
        for way in range(2):
            hop = len(REDUCE[piece % 2][way]) - 1
            here = rbuf_at(piece, way, hop)
            remote(here, here, ssem.at[piece, way, hop], rsem.at[piece, way, hop], sides[way]).wait_recv()
            total = total + here[...].astype(F32)
        return total

    args1 = (
        lambda p, s: part1.at[p, lax.rem(z - s + 8, 8)],
        lambda p, w, h: rbuf1.at[p, w, h],
        rs1_s,
        rs1_r,
    )
    for p in range(4):
        cols = pl.ds(512 * p, 512)
        prod = dot(xa[:, pl.ds(0, 128)], wa[0, :, cols]) + dot(xa[:, pl.ds(128, 128)], wa[1, :, cols])
        part1[p] = prod.astype(BF16).reshape(8, 32, 512)
        reduce_tick(0, (p,), *args1)
    e_duo = [
        send(gw_ref.at[0], wg.at[1], duo_s.at[2], duo_r.at[2], partner),
        send(uw_ref.at[0], wu.at[1], duo_s.at[3], duo_r.at[3], partner),
        send(dw_ref.at[0], wd.at[1], duo_s.at[4], duo_r.at[4], partner),
    ]

    def selections(axis, main, tails):
        shape = (192, 256) if axis == 0 else (256, 192)
        d, k, r = natural(iota(shape, axis))
        q = iota(shape, 1 - axis)
        same = (d == ((q >> 3) & 7)) & (k == (q >> 6))
        r8 = q & 7
        main[...] = jnp.where(same & (r8 == r), 1.0, 0.0).astype(BF16)
        for j in range(3):
            tails[j] = jnp.where(
                same & (((r8 == 6) & (r == j)) | ((r8 == 7) & (r == j + 3))), 1.0, 0.0
            ).astype(BF16)

    def tables(g):
        quarter = iota((8, 128), 1) >> 5
        m = jnp.zeros((8, 128), F32)
        for i, slot in enumerate(GROUPS[g]):
            m = jnp.where(quarter == i, meta[slot], m)
        d, k, r = natural(iota((384, 128), 0))
        lane = iota((384, 128), 1)
        d = d.astype(F32)
        first = jnp.broadcast_to(m[0:1, :], (384, 128)) == d
        second = jnp.broadcast_to(m[1:2, :], (384, 128)) == d
        named = (first | second).astype(F32)
        ta, tb = iota((128, 128), 0), iota((128, 128), 1)
        count = dot(named.astype(BF16), ((ta < tb) & ((ta >> 5) == (tb >> 5))).astype(BF16))
        table = jnp.where((count == r.astype(F32)) & (k == (lane >> 5)), named, 0.0)
        tdisp[g] = table.astype(BF16)
        for i in range(2):
            w = jnp.where(first, m[2 + 2 * i : 3 + 2 * i, :], m[3 + 2 * i : 4 + 2 * i, :])
            tcomb[g, i] = (table * w).astype(BF16)

    meta_tick(1)
    selections(0, gm, gt)
    reduce_tick(1, range(4), *args1)
    meta_tick(2)
    tables(0)
    reduce_tick(2, range(4), *args1)
    meta_tick(3)
    selections(1, gmt, gtt)
    reduce_tick(3, range(4), *args1)
    meta_tick(4)
    local[8].wait()
    local[9].wait()
    square = jnp.zeros((32, 1), F32)
    for p in range(4):
        cols = pl.ds(512 * p, 512)
        wide = (res_ref[:, cols].astype(F32) + reduce_last(p, *args1)).astype(BF16)
        hid[:, cols] = wide
        wide = wide.astype(F32)
        square = square + jnp.sum(wide * wide, axis=1, keepdims=True)
    scale = lax.rsqrt(square * (1.0 / 2048.0) + EPS)
    gain = gain_ref[...].astype(F32)
    for i in list(range(8, 16)) + list(range(8)):
        cols = pl.ds(128 * i, 128)
        nrm[:, cols] = (hid[:, cols].astype(F32) * scale * gain[i : i + 1, :]).astype(BF16)
    for c in range(2):
        tok[c, 0] = nrm[:, pl.ds(1024 + 512 * c, 512)]

    def tok_tick(k):
        for c in range(2):
            for way in range(2):
                slots = GATHER[c][way]
                if 0 < k <= len(slots):
                    slot = k if way == 0 else 8 - k
                    here = tok.at[c, slot]
                    remote(here, here, tok_s.at[c, slot], tok_r.at[c, slot], sides[way]).wait_recv()
                if k < len(slots):
                    to = (slots[k] + 1) % 8 if way == 0 else (slots[k] + 7) % 8
                    send(tok.at[c, slots[k]], tok.at[c, to], tok_s.at[c, to], tok_r.at[c, to], sides[way])

    tok_tick(0)

    tail = nrm[:, pl.ds(768, 256)]
    for j in range(3):
        cols = pl.ds(256 * j, 256)
        packed = (dot(tmain[...], nrm[:, cols]) + dot(ttail[j], tail)).astype(BF16)
        outg[:, :, cols] = packed.reshape(16, 8, 256)
    disp = {d: send(outg.at[d], xbuf.at[0, d], disp_s.at[d], disp_r.at[d], ahead(d)) for d in ORDER}
    xbuf[0, 0] = outg[0]

    def disp2(g):
        for c in range(2):
            cols = pl.ds(512 * c, 512)
            block = jnp.concatenate([tok[c, slot] for slot in GROUPS[g]], axis=0)
            out2[g, :, :, cols] = dot(tdisp[g], block).astype(BF16).reshape(16, 24, 512)
        for d in ORDER:
            came[g, d] = send(out2.at[g, d], x2buf.at[g, d], disp2_s.at[g, d], disp2_r.at[g, d], ahead(d))
        x2buf[g, 0] = out2[g, 0]

    came = {}

    def piece_at(buf, slot, piece):
        return buf.at[slot, pl.ds(4 * piece, 4)]

    def gather_tick(pair, k):
        for piece in (2 * pair, 2 * pair + 1):
            if k == 0:
                for d in range(4 * piece, 4 * piece + 4):
                    if d > 0:
                        disp[d].wait_recv()
            for way in range(2):
                slots = GATHER[piece % 2][way]
                if 0 < k <= len(slots):
                    slot = k if way == 0 else 8 - k
                    here = piece_at(xbuf, slot, piece)
                    remote(here, here, ag_s.at[piece, slot], ag_r.at[piece, slot], sides[way]).wait_recv()
                if k < len(slots):
                    to = (slots[k] + 1) % 8 if way == 0 else (slots[k] + 7) % 8
                    send(piece_at(xbuf, slots[k], piece), piece_at(xbuf, to, piece), ag_s.at[piece, to],
                         ag_r.at[piece, to], sides[way])

    def expert(pair, g):
        these = pl.ds(8 * pair, 8)
        for d in range(8 * pair, 8 * pair + 8):
            if d > 0:
                came[g, d].wait_recv()
        for i, slot in enumerate(GROUPS[g]):
            xcat[pl.ds(64 * i, 64), :] = xbuf[slot, these].reshape(64, 768)
        x2[:, pl.ds(0, 768)] = dot(gm[...], xcat[...]).astype(BF16)
        last = jnp.zeros((192, 256), F32)
        for j in range(3):
            last = last + dot(gt[j], xcat[:, pl.ds(256 * j, 256)])
        x2[:, pl.ds(768, 256)] = last.astype(BF16)
        x2[:, pl.ds(1024, 1024)] = x2buf[g, these].reshape(192, 1024)

        @pl.loop(0, 2)
        def _(h):
            gate = dot(x2[...], wg[h])
            up = dot(x2[...], wu[h])
            act[h] = (gate / (1.0 + jnp.exp(-gate)) * up).astype(BF16)

        def down(cols):
            return (dot(act[0], wd[0, :, cols]) + dot(act[1], wd[1, :, cols])).astype(BF16)

        @pl.loop(0, 2)
        def _(c):
            cols = pl.ds(pl.multiple_of(512 * c, 512), 512)
            y2[g, these, :, cols] = down(pl.ds(pl.multiple_of(1024 + 512 * c, 512), 512)).reshape(8, 24, 512)

        for d in ORDER:
            if d // 8 == pair:
                home[g, d] = send(y2.at[g, d], back2.at[g, d], ret2_s.at[g, d], ret2_r.at[g, d], behind(d))
        if pair == 0:
            back2[g, 0] = y2[g, 0]
        last = down(pl.ds(768, 256))

        @pl.loop(0, 3)
        def _(j):
            cols = pl.ds(pl.multiple_of(256 * j, 256), 256)
            packed = (dot(gmt[...], down(cols)) + dot(gtt[j], last)).astype(BF16)
            for i, slot in enumerate(GROUPS[g]):
                part[slot, these, :, cols] = packed[64 * i : 64 * i + 64].reshape(8, 8, 256)

    home = {}
    args = (
        lambda p, s: piece_at(part, s, p),
        lambda p, w, h: rbuf.at[p, w, h],
        rs_s,
        rs_r,
    )
    back = {}

    def send_back(pair):
        for piece in (2 * pair, 2 * pair + 1):
            fin[pl.ds(4 * piece, 4)] = reduce_last(piece, *args).astype(BF16)
            for d in range(4 * piece, 4 * piece + 4):
                if d == 0:
                    ret[0] = fin[0]
                else:
                    back[d] = send(fin.at[d], ret.at[d], ret_s.at[d], ret_r.at[d], behind(d))

    args2 = (
        lambda p, s: cpart.at[p, s],
        lambda p, w, h: rbuf2.at[p, w, h],
        rs2_s,
        rs2_r,
    )

    def combine(g):
        for d in range(1, 16):
            home[g, d].wait_recv()
        for c in range(2):
            block = back2[g, :, :, pl.ds(512 * c, 512)].reshape(384, 512)
            total = dot_t(tcomb[g, 0], block) + dot_t(tcomb[g, 1], block)
            for i, slot in enumerate(GROUPS[g]):
                cpart[c, slot] = total[32 * i : 32 * i + 32].astype(BF16)

    tables(1)
    tok_tick(1)
    gather_tick(0, 0)
    tok_tick(2)
    disp2(0)
    gather_tick(0, 1)
    tok_tick(3)
    gather_tick(0, 2)
    gather_tick(1, 0)
    tok_tick(4)
    disp2(1)
    gather_tick(0, 3)
    gather_tick(1, 1)
    for c in local[10:]:
        c.wait()
    for c in e_duo:
        c.wait_recv()
    expert(0, 0)
    gather_tick(0, 4)
    gather_tick(1, 2)
    gather_tick(1, 3)
    expert(0, 1)
    reduce_tick(0, (0, 1), *args)
    gather_tick(1, 4)
    reduce_tick(1, (0, 1), *args)
    expert(1, 1)
    reduce_tick(0, (2, 3), *args)
    reduce_tick(2, (0, 1), *args)
    expert(1, 0)
    reduce_tick(1, (2, 3), *args)
    reduce_tick(3, (0, 1), *args)
    combine(1)
    reduce_tick(0, (0, 1), *args2)
    reduce_tick(2, (2, 3), *args)
    send_back(0)
    reduce_tick(1, (0, 1), *args2)
    combine(0)
    reduce_tick(3, (2, 3), *args)
    reduce_tick(2, (0, 1), *args2)
    send_back(1)
    reduce_tick(3, (0, 1), *args2)

    for c in range(2):
        cols = pl.ds(1024 + 512 * c, 512)
        out_ref[:, cols] = (hid[:, cols].astype(F32) + reduce_last(c, *args2)).astype(BF16)
    for d in range(1, 16):
        back[d].wait_recv()
    weight = [
        jnp.where(one[0], line[i : i + 1, :], 0.0) + jnp.where(one[1], line[i + 1 : i + 2, :], 0.0) for i in (2, 4)
    ]
    weight = [w.astype(BF16) for w in weight]
    last = jnp.zeros((32, 256), F32)
    for j in range(3):
        cols = pl.ds(256 * j, 256)
        block = ret[:, :, cols].reshape(128, 256)
        acc = jnp.zeros((32, 256), F32)
        for w in weight:
            acc = acc + dot_t(w * tmain[...], block)
            last = last + dot_t(w * ttail[j], block)
        out_ref[:, cols] = (hid[:, cols].astype(F32) + acc).astype(BF16)
    cols = pl.ds(768, 256)
    out_ref[:, cols] = (hid[:, cols].astype(F32) + last).astype(BF16)
    for c in pending:
        c.wait_send()


def shards(
    out_gate, in_gate, conv_input, conv_taps, documents, out_weight, residual, norm_gain, expert_ids, route_weights,
    gate_weight, up_weight, down_weight,
):
    hbm = pl.BlockSpec(memory_space=pl.ANY)
    dma = pltpu.SemaphoreType.DMA

    def buf(*shape, dtype=BF16):
        return pltpu.VMEM(shape, dtype)

    scratch = [
        buf(512, 128), buf(512, 128), buf(512, 128), buf(3, 128), buf(4, 128, dtype=jnp.int32), buf(32, 2048),
        buf(16, 128), buf(2, 32, dtype=jnp.int32), buf(2, 32, dtype=F32),
        buf(16, 128), buf(16, 128), buf(4, 128, dtype=jnp.int32), buf(528, 128, dtype=F32), buf(528, 128, dtype=F32),
        buf(3, 256, 128), buf(256, 256), buf(2, 128, 2048), buf(4, 8, 32, 512), buf(4, 2, 4, 32, 512),
        buf(32, 2048), buf(32, 2048),
        buf(8, 32, dtype=F32), buf(8, 8, 128, dtype=F32), buf(128, 32), buf(3, 128, 32), buf(2, 384, 128),
        buf(2, 2, 384, 128), buf(192, 256), buf(3, 192, 256), buf(256, 192), buf(3, 256, 192),
        buf(2, 8, 32, 512), buf(16, 8, 768), buf(2, 16, 24, 1024), buf(8, 16, 8, 768), buf(2, 16, 24, 1024),
        buf(256, 768), buf(192, 2048), buf(2, 192, 256), buf(2, 2048, 256), buf(2, 2048, 256), buf(2, 256, 2048),
        buf(8, 16, 8, 768), buf(4, 2, 4, 4, 8, 768), buf(2, 16, 24, 1024), buf(2, 16, 24, 1024), buf(2, 8, 32, 512),
        buf(2, 2, 4, 32, 512), buf(16, 8, 768), buf(16, 8, 768),
        dma((13,)), dma((3,)), dma((3,)), dma((5,)), dma((5,)), dma((8,)), dma((8,)), dma((4, 2, 4)), dma((4, 2, 4)),
        dma((2, 8)), dma((2, 8)), dma((16,)), dma((16,)), dma((4, 8)), dma((4, 8)),
        dma((2, 16)), dma((2, 16)), dma((4, 2, 4)), dma((4, 2, 4)), dma((2, 16)), dma((2, 16)), dma((2, 2, 4)),
        dma((2, 2, 4)), dma((16,)), dma((16,)),
    ]
    return pl.pallas_call(
        kernel,
        out_shape=jax.ShapeDtypeStruct((32, 2048), BF16),
        in_specs=[hbm] * 13,
        out_specs=pl.BlockSpec(memory_space=pltpu.VMEM),
        scratch_shapes=scratch,
        compiler_params=pltpu.CompilerParams(
            collective_id=0, has_side_effects=True, vmem_limit_bytes=56 * 1024 * 1024
        ),
        name="layer",
    )(
        out_gate, in_gate, conv_input, conv_taps, documents.reshape(4, 128), out_weight, residual,
        norm_gain.reshape(16, 128), expert_ids.T, route_weights.T, gate_weight, up_weight, down_weight,
    )


def solution(mesh):
    in_specs = (
        P("sp", "tp"),
        P("sp", "tp"),
        P("sp", "tp"),
        P(None, "tp"),
        P("sp"),
        P("tp", None),
        P(("sp", "tp"), None),
        P(),
        P(("sp", "tp"), None),
        P(("sp", "tp"), None),
        P("sp", None, "tp"),
        P("sp", None, "tp"),
        P("sp", "tp", None),
    )
    out_specs = P(("sp", "tp"), None)
    return jax.shard_map(shards, mesh=mesh, in_specs=in_specs, out_specs=out_specs, check_vma=False)
```

```python
import jax
import jax.numpy as jnp
from jax import lax
from jax.experimental import pallas as pl
from jax.experimental.pallas import tpu as pltpu
from jax.sharding import PartitionSpec as P

EPS = 1e-06
MESH = pl.DeviceIdType.MESH
F32 = jnp.float32
BF16 = jnp.bfloat16

GATHER = {0: ((0, 1, 2, 3), (0, 7, 6)), 1: ((0, 1, 2), (0, 7, 6, 5))}
REDUCE = {0: ((4, 5, 6, 7), (3, 2, 1)), 1: ((5, 6, 7), (4, 3, 2, 1))}
GROUPS = ((0, 1, 7, 2), (6, 3, 5, 4))
DY = (0, 2, 1, 3)
ORDER = (6, 5, 7, 4, 2, 1, 3, 10, 14, 9, 11, 13, 15, 8, 12)


def dot(a, b):
    return jnp.dot(a, b, preferred_element_type=F32)


def dot_t(a, b):
    return lax.dot_general(a, b, (((0,), (0,)), ((), ())), preferred_element_type=F32)


def iota(shape, dim):
    return lax.broadcasted_iota(jnp.int32, shape, dim)


def natural(q):
    d = (q * 2731) >> 16
    rest = q - 24 * d
    k = (rest * 10923) >> 16
    return d, k, rest - 6 * k


def kernel(
    og_hbm, ig_hbm, ci_hbm, taps_hbm, docs_hbm, ow_ref, res_hbm, gain_hbm, ids_hbm, rw_hbm, gw_ref, uw_ref, dw_ref,
    out_ref,
    og_ref, ig_ref, ci_ref, taps_ref, docs_ref, res_ref, gain_ref, ids_ref, rw_ref,
    h_in, h_docs, ext, extd, gbuf, xa, wa, part1, rbuf1, hid, nrm,
    line, meta, tmain, ttail, tdisp, tcomb, gm, gt, gmt, gtt,
    tok, outg, out2, xbuf, x2buf, xcat, x2, act, wg, wu, wd, part, rbuf, y2, back2, cpart, rbuf2, fin, ret,
    loc_sem, out_sem, in_sem, meta_r, ag_r, rs_r, tok_r, ret_r,
):
    sp = lax.axis_index("sp")
    tp = lax.axis_index("tp")
    core = lax.rem(tp, 2)
    z = tp // 2
    y, x = sp // 4, lax.rem(sp, 4)
    right = {"tp": lax.rem(z + 1, 8) * 2 + core}
    left = {"tp": lax.rem(z + 7, 8) * 2 + core}
    sides = (right, left)
    partner = {"tp": z * 2 + 1 - core}
    following = {"sp": lax.rem(sp + 1, 16)}

    def ahead(d):
        return {"sp": lax.rem(y + DY[d // 4], 4) * 4 + lax.rem(x + d % 4, 4)}

    def behind(d):
        return {"sp": lax.rem(y + 4 - DY[d // 4], 4) * 4 + lax.rem(x + 4 - d % 4, 4)}

    def remote(src, dst, ssem, rsem, device):
        return pltpu.make_async_remote_copy(
            src_ref=src, dst_ref=dst, send_sem=ssem, recv_sem=rsem, device_id=device, device_id_type=MESH
        )

    def send(*args):
        c = remote(*args)
        c.start()
        return c

    def sent(ref, i):
        remote(ref, ref, out_sem.at[i], in_sem.at[0], right).wait_send()

    def received(ref, sem):
        remote(ref, ref, out_sem.at[0], sem, right).wait_recv()

    barrier = pltpu.get_barrier_semaphore()
    for device in [right, left, partner]:
        pl.semaphore_signal(barrier, inc=1, device_id=device, device_id_type=MESH)
    for d in range(1, 16):
        pl.semaphore_signal(barrier, inc=1, device_id=ahead(d), device_id_type=MESH)

    pairs = [
        (ids_hbm, ids_ref), (rw_hbm, rw_ref), (ig_hbm, ig_ref), (ci_hbm, ci_ref), (docs_hbm, docs_ref),
        (taps_hbm, taps_ref), (og_hbm, og_ref), (ow_ref, wa.at[0]), (res_hbm, res_ref), (gain_hbm, gain_ref),
        (gw_ref.at[0], wg.at[0]), (uw_ref.at[0], wu.at[0]), (dw_ref.at[0], wd.at[0]),
    ]
    local = [pltpu.make_async_copy(a, b, loc_sem.at[i]) for i, (a, b) in enumerate(pairs)]
    for c in local:
        c.start()

    local[0].wait()
    local[1].wait()
    ids = ids_ref[...]
    dy = ((ids >> 2) - y + 4) & 3
    rid = ((dy >> 1) + 2 * (dy & 1)) * 4 + (((ids & 3) - x + 4) & 3)
    weight = rw_ref[...]
    high = weight.astype(BF16).astype(F32)
    line[pl.ds(0, 2), :] = rid.astype(F32)
    line[pl.ds(2, 2), :] = high
    line[pl.ds(4, 2), :] = (weight - high).astype(BF16).astype(F32)
    line[pl.ds(6, 2), :] = jnp.zeros((2, 32), F32)
    spread = (iota((32, 128), 0) == (iota((32, 128), 1) & 31)).astype(BF16)
    meta[0] = dot(line[...].astype(BF16), spread)

    local[2].wait()
    local[3].wait()
    local[4].wait()
    local[5].wait()
    local[6].wait()
    ext[pl.ds(16, 512), :] = ig_ref[...].astype(F32) * ci_ref[...].astype(F32)
    docs = docs_ref[...].astype(F32)
    for i in range(4):
        extd[pl.ds(16 + 128 * i, 128), :] = jnp.broadcast_to(docs[i : i + 1, :], (128, 128)).T
    taps = taps_ref[...].astype(F32)

    def gated(first, count):
        pos = sp * 512 + first + iota((count, 128), 0)
        now = extd[pl.ds(16 + first, count), :]
        conv = taps[2:3, :] * ext[pl.ds(16 + first, count), :]
        for off in (1, 2):
            ok = (pos >= off) & (extd[pl.ds(16 + first - off, count), :] == now)
            earlier = taps[2 - off : 3 - off, :] * ext[pl.ds(16 + first - off, count), :]
            conv = conv + jnp.where(ok, earlier, 0.0)
        return (og_ref[pl.ds(first, count), :].astype(F32) * conv).astype(BF16)

    for j in range(1, 16):
        gbuf[j % 2, pl.ds(32 * (j // 2), 32), :] = gated(32 * j, 32)

    pl.semaphore_wait(barrier, 18)

    send(ig_ref.at[pl.ds(496, 16)], h_in.at[0], out_sem.at[0], in_sem.at[0], following)
    send(ci_ref.at[pl.ds(496, 16)], h_in.at[1], out_sem.at[0], in_sem.at[0], following)
    send(docs_ref, h_docs, out_sem.at[1], in_sem.at[1], following)
    rest = pl.ds(32, 224)
    g_duo = [send(gbuf.at[1 - core, rest], gbuf.at[2, rest], out_sem.at[2], in_sem.at[2], partner)]
    local[7].wait()
    w_duo = send(wa.at[0], wa.at[1], out_sem.at[3], in_sem.at[3], partner)

    e_duo = [
        send(gw_ref.at[0], wg.at[1], out_sem.at[7], in_sem.at[5], partner),
        send(uw_ref.at[0], wu.at[1], out_sem.at[8], in_sem.at[6], partner),
    ]

    def meta_tick(k):
        for way in range(2):
            slots = GATHER[0][way]
            if 0 < k <= len(slots):
                slot = k if way == 0 else 8 - k
                received(meta.at[slot], meta_r.at[slot - 1])
            if k < len(slots):
                to = (slots[k] + 1) % 8 if way == 0 else (slots[k] + 7) % 8
                send(meta.at[slots[k]], meta.at[to], out_sem.at[4], meta_r.at[to - 1], sides[way])

    meta_tick(0)
    received(h_in, in_sem.at[0])
    received(h_docs, in_sem.at[1])
    ext[pl.ds(0, 16), :] = h_in[0].astype(F32) * h_in[1].astype(F32)
    old = jnp.broadcast_to(h_docs[...].astype(F32)[3:4, :], (128, 128)).T
    extd[pl.ds(0, 16), :] = old[112:128, :]
    gbuf[0, pl.ds(0, 32), :] = gated(0, 32)
    rest = pl.ds(0, 32)
    g_duo.append(send(gbuf.at[1 - core, rest], gbuf.at[2, rest], out_sem.at[5], in_sem.at[4], partner))
    e_duo.append(send(dw_ref.at[0], wd.at[1], out_sem.at[9], in_sem.at[7], partner))
    xa[:, pl.ds(0, 128)] = gbuf[core]

    rows = iota((128, 32), 0)
    rel, sub = rows >> 3, (rows & 7).astype(F32)
    one = [(jnp.broadcast_to(rid[k : k + 1, :], (128, 32)) == rel) for k in range(2)]
    both = (one[0] | one[1]).astype(F32)
    before = (iota((32, 32), 0) < iota((32, 32), 1)).astype(BF16)
    place = dot(both.astype(BF16), before)
    tmain[...] = (jnp.where((place == sub) & (sub < 6.0), 1.0, 0.0) * both).astype(BF16)
    for j in range(3):
        hit = ((sub == 6.0) & (place == float(j))) | ((sub == 7.0) & (place == j + 3.0))
        ttail[j] = (jnp.where(hit, 1.0, 0.0) * both).astype(BF16)

    w_duo.wait_recv()
    for c in g_duo:
        c.wait_recv()
    xa[:, pl.ds(128, 128)] = gbuf[2]

    def arrival(rsem, piece, way, hop):
        return rsem.at[piece, hop if way == 0 else len(REDUCE[piece % 2][0]) + hop]

    def reduce_hop(piece, way, hop, part_at, rbuf_at, ssem, rsem):
        slots = REDUCE[piece % 2][way]
        here = part_at(piece, slots[hop])
        if hop > 0:
            came = rbuf_at(piece, way, hop - 1)
            received(came, arrival(rsem, piece, way, hop - 1))
            here[...] = (here[...].astype(F32) + came[...].astype(F32)).astype(BF16)
        send(here, rbuf_at(piece, way, hop), ssem, arrival(rsem, piece, way, hop), sides[way])

    def reduce_tick(t, pieces, *rest):
        for piece in pieces:
            for way in range(2):
                hop = t - (4 - len(REDUCE[piece % 2][way]))
                if hop >= 0:
                    reduce_hop(piece, way, hop, *rest)

    def reduce_last(piece, part_at, rbuf_at, ssem, rsem):
        total = part_at(piece, 0)[...].astype(F32)
        for way in range(2):
            hop = len(REDUCE[piece % 2][way]) - 1
            here = rbuf_at(piece, way, hop)
            received(here, arrival(rsem, piece, way, hop))
            total = total + here[...].astype(F32)
        return total

    args1 = (
        lambda p, s: part1.at[p, lax.rem(z - s + 8, 8)],
        lambda p, w, h: rbuf1.at[p, w, h],
        out_sem.at[6],
        rs_r,
    )
    for p in range(4):
        cols = pl.ds(512 * p, 512)
        prod = dot(xa[:, pl.ds(0, 128)], wa[0, :, cols]) + dot(xa[:, pl.ds(128, 128)], wa[1, :, cols])
        part1[p] = prod.astype(BF16).reshape(8, 32, 512)
        reduce_tick(0, (p,), *args1)
    def selections(axis, main, tails):
        shape = (192, 256) if axis == 0 else (256, 192)
        d, k, r = natural(iota(shape, axis))
        q = iota(shape, 1 - axis)
        same = (d == ((q >> 3) & 7)) & (k == (q >> 6))
        r8 = q & 7
        main[...] = jnp.where(same & (r8 == r), 1.0, 0.0).astype(BF16)
        for j in range(3):
            tails[j] = jnp.where(
                same & (((r8 == 6) & (r == j)) | ((r8 == 7) & (r == j + 3))), 1.0, 0.0
            ).astype(BF16)

    def tables(g):
        quarter = iota((8, 128), 1) >> 5
        m = jnp.zeros((8, 128), F32)
        for i, slot in enumerate(GROUPS[g]):
            m = jnp.where(quarter == i, meta[slot], m)
        d, k, r = natural(iota((384, 128), 0))
        lane = iota((384, 128), 1)
        d = d.astype(F32)
        first = jnp.broadcast_to(m[0:1, :], (384, 128)) == d
        second = jnp.broadcast_to(m[1:2, :], (384, 128)) == d
        named = (first | second).astype(F32)
        ta, tb = iota((128, 128), 0), iota((128, 128), 1)
        count = dot(named.astype(BF16), ((ta < tb) & ((ta >> 5) == (tb >> 5))).astype(BF16))
        table = jnp.where((count == r.astype(F32)) & (k == (lane >> 5)), named, 0.0)
        tdisp[g] = table.astype(BF16)
        for i in range(2):
            w = jnp.where(first, m[2 + 2 * i : 3 + 2 * i, :], m[3 + 2 * i : 4 + 2 * i, :])
            tcomb[g, i] = (table * w).astype(BF16)

    meta_tick(1)
    selections(0, gm, gt)
    reduce_tick(1, range(4), *args1)
    meta_tick(2)
    tables(0)
    reduce_tick(2, range(4), *args1)
    meta_tick(3)
    selections(1, gmt, gtt)
    reduce_tick(3, range(4), *args1)
    meta_tick(4)
    local[8].wait()
    local[9].wait()
    square = jnp.zeros((32, 1), F32)
    for p in range(4):
        cols = pl.ds(512 * p, 512)
        wide = (res_ref[:, cols].astype(F32) + reduce_last(p, *args1)).astype(BF16)
        hid[:, cols] = wide
        wide = wide.astype(F32)
        square = square + jnp.sum(wide * wide, axis=1, keepdims=True)
    scale = lax.rsqrt(square * (1.0 / 2048.0) + EPS)
    gain = gain_ref[...].astype(F32)
    for i in list(range(8, 16)) + list(range(8)):
        cols = pl.ds(128 * i, 128)
        nrm[:, cols] = (hid[:, cols].astype(F32) * scale * gain[i : i + 1, :]).astype(BF16)
    for c in range(2):
        tok[c, 0] = nrm[:, pl.ds(1024 + 512 * c, 512)]

    def tok_tick(k):
        for c in range(2):
            for way in range(2):
                slots = GATHER[c][way]
                if 0 < k <= len(slots):
                    slot = k if way == 0 else 8 - k
                    received(tok.at[c, slot], tok_r.at[c, slot - 1])
                if k < len(slots):
                    to = (slots[k] + 1) % 8 if way == 0 else (slots[k] + 7) % 8
                    send(tok.at[c, slots[k]], tok.at[c, to], out_sem.at[10], tok_r.at[c, to - 1], sides[way])

    tok_tick(0)

    tail = nrm[:, pl.ds(768, 256)]
    for j in range(3):
        cols = pl.ds(256 * j, 256)
        packed = (dot(tmain[...], nrm[:, cols]) + dot(ttail[j], tail)).astype(BF16)
        outg[:, :, cols] = packed.reshape(16, 8, 256)
    for d in ORDER:
        send(outg.at[d], xbuf.at[0, d], out_sem.at[11], in_sem.at[8 + d // 8], ahead(d))
    xbuf[0, 0] = outg[0]

    def disp2(g):
        for c in range(2):
            cols = pl.ds(512 * c, 512)
            block = jnp.concatenate([tok[c, slot] for slot in GROUPS[g]], axis=0)
            out2[g, :, :, cols] = dot(tdisp[g], block).astype(BF16).reshape(16, 24, 512)
        for d in ORDER:
            send(out2.at[g, d], x2buf.at[g, d], out_sem.at[12 + g], in_sem.at[10 + 2 * g + d // 8], ahead(d))
        x2buf[g, 0] = out2[g, 0]

    def piece_at(buf, slot, piece):
        return buf.at[slot, pl.ds(4 * piece, 4)]

    def whole(pair):
        return pl.ds(8, 8) if pair else pl.ds(1, 7)

    def gather_tick(pair, k):
        if k == 0:
            received(xbuf.at[0, whole(pair)], in_sem.at[8 + pair])
        for piece in (2 * pair, 2 * pair + 1):
            for way in range(2):
                slots = GATHER[piece % 2][way]
                if 0 < k <= len(slots):
                    slot = k if way == 0 else 8 - k
                    received(piece_at(xbuf, slot, piece), ag_r.at[piece, slot - 1])
                if k < len(slots):
                    to = (slots[k] + 1) % 8 if way == 0 else (slots[k] + 7) % 8
                    send(piece_at(xbuf, slots[k], piece), piece_at(xbuf, to, piece), out_sem.at[14],
                         ag_r.at[piece, to - 1], sides[way])

    def expert(pair, g, step):
        these = pl.ds(8 * pair, 8)

        def down(cols):
            return (dot(act[0], wd[0, :, cols]) + dot(act[1], wd[1, :, cols])).astype(BF16)

        if step == 0:
            for i, slot in enumerate(GROUPS[g]):
                xcat[pl.ds(64 * i, 64), :] = xbuf[slot, these].reshape(64, 768)
            x2[:, pl.ds(0, 768)] = dot(gm[...], xcat[...]).astype(BF16)
            last = jnp.zeros((192, 256), F32)
            for j in range(3):
                last = last + dot(gt[j], xcat[:, pl.ds(256 * j, 256)])
            x2[:, pl.ds(768, 256)] = last.astype(BF16)
            received(x2buf.at[g, whole(pair)], in_sem.at[10 + 2 * g + pair])
            x2[:, pl.ds(1024, 1024)] = x2buf[g, these].reshape(192, 1024)
        if step < 2:
            gate = dot(x2[...], wg[step])
            up = dot(x2[...], wu[step])
            act[step] = (gate / (1.0 + jnp.exp(-gate)) * up).astype(BF16)
        if step == 2:
            for c in range(2):
                y2[g, these, :, pl.ds(512 * c, 512)] = down(pl.ds(1024 + 512 * c, 512)).reshape(8, 24, 512)

            for d in ORDER:
                if d // 8 == pair:
                    send(y2.at[g, d], back2.at[g, d], out_sem.at[15], in_sem.at[14 + g], behind(d))
            if pair == 0:
                back2[g, 0] = y2[g, 0]
        if step == 3:
            last = down(pl.ds(768, 256))
            for j in range(3):
                cols = pl.ds(256 * j, 256)
                packed = (dot(gmt[...], down(cols)) + dot(gtt[j], last)).astype(BF16)
                for i, slot in enumerate(GROUPS[g]):
                    part[slot, these, :, cols] = packed[64 * i : 64 * i + 64].reshape(8, 8, 256)

    args = (
        lambda p, s: piece_at(part, s, p),
        lambda p, w, h: rbuf.at[p, w, h],
        out_sem.at[16],
        rs_r,
    )

    def send_back(pair):
        for piece in (2 * pair, 2 * pair + 1):
            fin[pl.ds(4 * piece, 4)] = reduce_last(piece, *args).astype(BF16)
            for d in range(4 * piece, 4 * piece + 4):
                if d == 0:
                    ret[0] = fin[0]
                else:
                    send(fin.at[d], ret.at[d], out_sem.at[17], ret_r, behind(d))

    args2 = (
        lambda p, s: cpart.at[p, s],
        lambda p, w, h: rbuf2.at[p, w, h],
        out_sem.at[18],
        tok_r,
    )

    def combine(g):
        received(back2.at[g, pl.ds(1, 15)], in_sem.at[14 + g])
        for c in range(2):
            block = back2[g, :, :, pl.ds(512 * c, 512)].reshape(384, 512)
            total = dot_t(tcomb[g, 0], block) + dot_t(tcomb[g, 1], block)
            for i, slot in enumerate(GROUPS[g]):
                cpart[c, slot] = total[32 * i : 32 * i + 32].astype(BF16)

    tables(1)
    tok_tick(1)
    gather_tick(0, 0)
    tok_tick(2)
    disp2(0)
    gather_tick(0, 1)
    tok_tick(3)
    gather_tick(0, 2)
    gather_tick(1, 0)
    tok_tick(4)
    disp2(1)
    for c in local[10:]:
        c.wait()
    for c in e_duo:
        c.wait_recv()
    expert(0, 0, 0)
    gather_tick(0, 3)
    gather_tick(1, 1)
    expert(0, 0, 1)
    expert(0, 0, 2)
    gather_tick(0, 4)
    gather_tick(1, 2)
    expert(0, 0, 3)
    expert(0, 1, 0)
    gather_tick(1, 3)
    expert(0, 1, 1)
    expert(0, 1, 2)
    expert(0, 1, 3)
    reduce_tick(0, (0, 1), *args)
    gather_tick(1, 4)
    expert(1, 1, 0)
    expert(1, 1, 1)
    expert(1, 1, 2)
    reduce_tick(1, (0, 1), *args)
    expert(1, 1, 3)
    reduce_tick(0, (2, 3), *args)
    expert(1, 0, 0)
    reduce_tick(2, (0, 1), *args)
    expert(1, 0, 1)
    expert(1, 0, 2)
    reduce_tick(3, (0, 1), *args)
    expert(1, 0, 3)
    reduce_tick(1, (2, 3), *args)
    combine(1)
    reduce_tick(0, (0, 1), *args2)
    send_back(0)
    reduce_tick(2, (2, 3), *args)
    combine(0)
    reduce_tick(1, (0, 1), *args2)
    reduce_tick(3, (2, 3), *args)
    reduce_tick(2, (0, 1), *args2)
    send_back(1)
    reduce_tick(3, (0, 1), *args2)

    for c in range(2):
        cols = pl.ds(1024 + 512 * c, 512)
        out_ref[:, cols] = (hid[:, cols].astype(F32) + reduce_last(c, *args2)).astype(BF16)
    received(ret.at[pl.ds(1, 15)], ret_r)
    weight = [
        jnp.where(one[0], line[i : i + 1, :], 0.0) + jnp.where(one[1], line[i + 1 : i + 2, :], 0.0) for i in (2, 4)
    ]
    weight = [w.astype(BF16) for w in weight]
    last = jnp.zeros((32, 256), F32)
    for j in range(3):
        cols = pl.ds(256 * j, 256)
        block = ret[:, :, cols].reshape(128, 256)
        acc = jnp.zeros((32, 256), F32)
        for w in weight:
            acc = acc + dot_t(w * tmain[...], block)
            last = last + dot_t(w * ttail[j], block)
        out_ref[:, cols] = (hid[:, cols].astype(F32) + acc).astype(BF16)
    cols = pl.ds(768, 256)
    out_ref[:, cols] = (hid[:, cols].astype(F32) + last).astype(BF16)
    sent(h_in, 0)
    sent(h_docs, 1)
    for c in g_duo + [w_duo] + e_duo:
        c.wait_send()
    sent(meta.at[pl.ds(1, 7)], 4)
    sent(part1.at[:, pl.ds(1, 7)], 6)
    sent(tok.at[:, pl.ds(1, 7)], 10)
    sent(outg.at[pl.ds(1, 15)], 11)
    sent(out2.at[0, pl.ds(1, 15)], 12)
    sent(out2.at[1, pl.ds(1, 15)], 13)
    sent(xbuf.at[pl.ds(1, 7)], 14)
    sent(y2.at[:, pl.ds(1, 15)], 15)
    sent(part.at[pl.ds(1, 7)], 16)
    sent(fin.at[pl.ds(1, 15)], 17)
    sent(cpart.at[:, pl.ds(1, 7)], 18)


def shards(
    out_gate, in_gate, conv_input, conv_taps, documents, out_weight, residual, norm_gain, expert_ids, route_weights,
    gate_weight, up_weight, down_weight,
):
    hbm = pl.BlockSpec(memory_space=pl.ANY)
    dma = pltpu.SemaphoreType.DMA

    def buf(*shape, dtype=BF16):
        return pltpu.VMEM(shape, dtype)

    scratch = [
        buf(512, 128), buf(512, 128), buf(512, 128), buf(3, 128), buf(4, 128, dtype=jnp.int32), buf(32, 2048),
        buf(16, 128), buf(2, 32, dtype=jnp.int32), buf(2, 32, dtype=F32),
        buf(2, 16, 128), buf(4, 128, dtype=jnp.int32), buf(528, 128, dtype=F32), buf(528, 128, dtype=F32),
        buf(3, 256, 128), buf(256, 256), buf(2, 128, 2048), buf(4, 8, 32, 512), buf(4, 2, 4, 32, 512),
        buf(32, 2048), buf(32, 2048),
        buf(8, 32, dtype=F32), buf(8, 8, 128, dtype=F32), buf(128, 32), buf(3, 128, 32), buf(2, 384, 128),
        buf(2, 2, 384, 128), buf(192, 256), buf(3, 192, 256), buf(256, 192), buf(3, 256, 192),
        buf(2, 8, 32, 512), buf(16, 8, 768), buf(2, 16, 24, 1024), buf(8, 16, 8, 768), buf(2, 16, 24, 1024),
        buf(256, 768), buf(192, 2048), buf(2, 192, 256), buf(2, 2048, 256), buf(2, 2048, 256), buf(2, 256, 2048),
        buf(8, 16, 8, 768), buf(4, 2, 4, 4, 8, 768), buf(2, 16, 24, 1024), buf(2, 16, 24, 1024), buf(2, 8, 32, 512),
        buf(2, 2, 4, 32, 512), buf(16, 8, 768), buf(16, 8, 768),
        dma((13,)), dma((19,)), dma((16,)), dma((7,)), dma((4, 7)), dma((4, 7)), dma((2, 7)), dma,
    ]
    return pl.pallas_call(
        kernel,
        out_shape=jax.ShapeDtypeStruct((32, 2048), BF16),
        in_specs=[hbm] * 13,
        out_specs=pl.BlockSpec(memory_space=pltpu.VMEM),
        scratch_shapes=scratch,
        compiler_params=pltpu.CompilerParams(
            collective_id=0, has_side_effects=True, vmem_limit_bytes=56 * 1024 * 1024
        ),
        name="layer",
    )(
        out_gate, in_gate, conv_input, conv_taps, documents.reshape(4, 128), out_weight, residual,
        norm_gain.reshape(16, 128), expert_ids.T, route_weights.T, gate_weight, up_weight, down_weight,
    )


def solution(mesh):
    in_specs = (
        P("sp", "tp"),
        P("sp", "tp"),
        P("sp", "tp"),
        P(None, "tp"),
        P("sp"),
        P("tp", None),
        P(("sp", "tp"), None),
        P(),
        P(("sp", "tp"), None),
        P(("sp", "tp"), None),
        P("sp", None, "tp"),
        P("sp", None, "tp"),
        P("sp", "tp", None),
    )
    out_specs = P(("sp", "tp"), None)
    return jax.shard_map(shards, mesh=mesh, in_specs=in_specs, out_specs=out_specs, check_vma=False)
```

```python
import jax
import jax.numpy as jnp
from jax import lax
from jax.experimental import pallas as pl
from jax.experimental.pallas import tpu as pltpu
from jax.sharding import PartitionSpec as P

EPS = 1e-06
MESH = pl.DeviceIdType.MESH
F32 = jnp.float32
BF16 = jnp.bfloat16

GATHER = {0: ((0, 1, 2, 3), (0, 7, 6)), 1: ((0, 1, 2), (0, 7, 6, 5))}
REDUCE = {0: ((4, 5, 6, 7), (3, 2, 1)), 1: ((5, 6, 7), (4, 3, 2, 1))}
GROUPS = ((0, 1, 7, 2), (6, 3, 5, 4))
DY = (0, 2, 1, 3)
ORDER = (6, 5, 7, 4, 2, 1, 3, 10, 14, 9, 11, 13, 15, 8, 12)


def dot(a, b):
    return jnp.dot(a, b, preferred_element_type=F32)


def dot_t(a, b):
    return lax.dot_general(a, b, (((0,), (0,)), ((), ())), preferred_element_type=F32)


def iota(shape, dim):
    return lax.broadcasted_iota(jnp.int32, shape, dim)


def natural(q):
    d = (q * 2731) >> 16
    rest = q - 24 * d
    k = (rest * 10923) >> 16
    return d, k, rest - 6 * k


def kernel(
    og_hbm, ig_hbm, ci_hbm, taps_hbm, docs_hbm, ow_ref, res_hbm, gain_hbm, ids_hbm, rw_hbm, gw_ref, uw_ref, dw_ref,
    out_ref,
    og_ref, ig_ref, ci_ref, taps_ref, docs_ref, res_ref, gain_ref, ids_ref, rw_ref,
    h_in, h_docs, ext, extd, gbuf, xa, wa, part1, rbuf1, hid, nrm,
    line, meta, tmain, ttail, tdisp, tcomb, gm, gt, gmt, gtt,
    tok, outg, out2, xbuf, x2buf, xcat, x2, act, wg, wu, wd, part, rbuf, y2, back2, cpart, rbuf2, fin, ret,
    loc_sem, out_sem, in_sem, meta_r, ag_r, rs_r, tok_r, ret_r,
):
    sp = lax.axis_index("sp")
    tp = lax.axis_index("tp")
    core = lax.rem(tp, 2)
    z = tp // 2
    y, x = sp // 4, lax.rem(sp, 4)
    right = {"tp": lax.rem(z + 1, 8) * 2 + core}
    left = {"tp": lax.rem(z + 7, 8) * 2 + core}
    sides = (right, left)
    partner = {"tp": z * 2 + 1 - core}
    following = {"sp": lax.rem(sp + 1, 16)}

    def ahead(d):
        return {"sp": lax.rem(y + DY[d // 4], 4) * 4 + lax.rem(x + d % 4, 4)}

    def behind(d):
        return {"sp": lax.rem(y + 4 - DY[d // 4], 4) * 4 + lax.rem(x + 4 - d % 4, 4)}

    def remote(src, dst, ssem, rsem, device):
        return pltpu.make_async_remote_copy(
            src_ref=src, dst_ref=dst, send_sem=ssem, recv_sem=rsem, device_id=device, device_id_type=MESH
        )

    def send(*args):
        c = remote(*args)
        c.start()
        return c

    def sent(ref, i):
        remote(ref, ref, out_sem.at[i], in_sem.at[0], right).wait_send()

    def received(ref, sem):
        remote(ref, ref, out_sem.at[0], sem, right).wait_recv()

    barrier = pltpu.get_barrier_semaphore()
    for device in [right, left, partner]:
        pl.semaphore_signal(barrier, inc=1, device_id=device, device_id_type=MESH)
    for d in range(1, 16):
        pl.semaphore_signal(barrier, inc=1, device_id=ahead(d), device_id_type=MESH)

    pairs = [
        (ids_hbm, ids_ref), (rw_hbm, rw_ref), (ig_hbm, ig_ref), (ci_hbm, ci_ref), (docs_hbm, docs_ref),
        (taps_hbm, taps_ref), (og_hbm, og_ref), (ow_ref, wa.at[0]), (res_hbm, res_ref), (gain_hbm, gain_ref),
        (gw_ref.at[0], wg.at[0]), (uw_ref.at[0], wu.at[0]), (dw_ref.at[0], wd.at[0]),
    ]
    local = [pltpu.make_async_copy(a, b, loc_sem.at[i]) for i, (a, b) in enumerate(pairs)]
    for c in local:
        c.start()

    local[0].wait()
    local[1].wait()
    ids = ids_ref[...]
    dy = ((ids >> 2) - y + 4) & 3
    rid = ((dy >> 1) + 2 * (dy & 1)) * 4 + (((ids & 3) - x + 4) & 3)
    weight = rw_ref[...]
    high = weight.astype(BF16).astype(F32)
    line[pl.ds(0, 2), :] = rid.astype(F32)
    line[pl.ds(2, 2), :] = high
    line[pl.ds(4, 2), :] = (weight - high).astype(BF16).astype(F32)
    line[pl.ds(6, 2), :] = jnp.zeros((2, 32), F32)
    spread = (iota((32, 128), 0) == (iota((32, 128), 1) & 31)).astype(BF16)
    meta[0] = dot(line[...].astype(BF16), spread)

    local[2].wait()
    local[3].wait()
    local[4].wait()
    local[5].wait()
    local[6].wait()
    ext[pl.ds(16, 512), :] = ig_ref[...].astype(F32) * ci_ref[...].astype(F32)
    docs = docs_ref[...].astype(F32)
    for i in range(4):
        extd[pl.ds(16 + 128 * i, 128), :] = jnp.broadcast_to(docs[i : i + 1, :], (128, 128)).T
    taps = taps_ref[...].astype(F32)

    def gated(first, count):
        pos = sp * 512 + first + iota((count, 128), 0)
        now = extd[pl.ds(16 + first, count), :]
        conv = taps[2:3, :] * ext[pl.ds(16 + first, count), :]
        for off in (1, 2):
            ok = (pos >= off) & (extd[pl.ds(16 + first - off, count), :] == now)
            earlier = taps[2 - off : 3 - off, :] * ext[pl.ds(16 + first - off, count), :]
            conv = conv + jnp.where(ok, earlier, 0.0)
        return (og_ref[pl.ds(first, count), :].astype(F32) * conv).astype(BF16)

    for j in range(1, 16):
        gbuf[j % 2, pl.ds(32 * (j // 2), 32), :] = gated(32 * j, 32)

    pl.semaphore_wait(barrier, 18)

    send(ig_ref.at[pl.ds(496, 16)], h_in.at[0], out_sem.at[0], in_sem.at[0], following)
    send(ci_ref.at[pl.ds(496, 16)], h_in.at[1], out_sem.at[0], in_sem.at[0], following)
    send(docs_ref, h_docs, out_sem.at[1], in_sem.at[1], following)
    rest = pl.ds(32, 224)
    g_duo = [send(gbuf.at[1 - core, rest], gbuf.at[2, rest], out_sem.at[2], in_sem.at[2], partner)]
    local[7].wait()
    w_duo = send(wa.at[0], wa.at[1], out_sem.at[3], in_sem.at[3], partner)

    e_duo = [
        send(gw_ref.at[0], wg.at[1], out_sem.at[7], in_sem.at[5], partner),
        send(uw_ref.at[0], wu.at[1], out_sem.at[8], in_sem.at[6], partner),
    ]

    def meta_tick(k):
        for way in range(2):
            slots = GATHER[0][way]
            if 0 < k <= len(slots):
                slot = k if way == 0 else 8 - k
                received(meta.at[slot], meta_r.at[slot - 1])
            if k < len(slots):
                to = (slots[k] + 1) % 8 if way == 0 else (slots[k] + 7) % 8
                send(meta.at[slots[k]], meta.at[to], out_sem.at[4], meta_r.at[to - 1], sides[way])

    meta_tick(0)
    received(h_in, in_sem.at[0])
    received(h_docs, in_sem.at[1])
    ext[pl.ds(0, 16), :] = h_in[0].astype(F32) * h_in[1].astype(F32)
    old = jnp.broadcast_to(h_docs[...].astype(F32)[3:4, :], (128, 128)).T
    extd[pl.ds(0, 16), :] = old[112:128, :]
    gbuf[0, pl.ds(0, 32), :] = gated(0, 32)
    rest = pl.ds(0, 32)
    g_duo.append(send(gbuf.at[1 - core, rest], gbuf.at[2, rest], out_sem.at[5], in_sem.at[4], partner))
    e_duo.append(send(dw_ref.at[0], wd.at[1], out_sem.at[9], in_sem.at[7], partner))
    xa[:, pl.ds(0, 128)] = gbuf[core]

    rows = iota((128, 32), 0)
    rel, sub = rows >> 3, (rows & 7).astype(F32)
    one = [(jnp.broadcast_to(rid[k : k + 1, :], (128, 32)) == rel) for k in range(2)]
    both = (one[0] | one[1]).astype(F32)
    before = (iota((32, 32), 0) < iota((32, 32), 1)).astype(BF16)
    place = dot(both.astype(BF16), before)
    tmain[...] = (jnp.where((place == sub) & (sub < 6.0), 1.0, 0.0) * both).astype(BF16)
    for j in range(3):
        hit = ((sub == 6.0) & (place == float(j))) | ((sub == 7.0) & (place == j + 3.0))
        ttail[j] = (jnp.where(hit, 1.0, 0.0) * both).astype(BF16)

    w_duo.wait_recv()
    for c in g_duo:
        c.wait_recv()
    xa[:, pl.ds(128, 128)] = gbuf[2]

    def arrival(rsem, piece, way, hop):
        return rsem.at[piece, hop if way == 0 else len(REDUCE[piece % 2][0]) + hop]

    def reduce_hop(piece, way, hop, part_at, rbuf_at, ssem, rsem):
        slots = REDUCE[piece % 2][way]
        here = part_at(piece, slots[hop])
        if hop > 0:
            came = rbuf_at(piece, way, hop - 1)
            received(came, arrival(rsem, piece, way, hop - 1))
            here[...] = (here[...].astype(F32) + came[...].astype(F32)).astype(BF16)
        send(here, rbuf_at(piece, way, hop), ssem, arrival(rsem, piece, way, hop), sides[way])

    def reduce_tick(t, pieces, *rest):
        for piece in pieces:
            for way in range(2):
                if t < len(REDUCE[piece % 2][way]):
                    reduce_hop(piece, way, t, *rest)

    def reduce_last(piece, part_at, rbuf_at, ssem, rsem):
        total = part_at(piece, 0)[...].astype(F32)
        for way in range(2):
            hop = len(REDUCE[piece % 2][way]) - 1
            here = rbuf_at(piece, way, hop)
            received(here, arrival(rsem, piece, way, hop))
            total = total + here[...].astype(F32)
        return total

    args1 = (
        lambda p, s: part1.at[p, lax.rem(z - s + 8, 8)],
        lambda p, w, h: rbuf1.at[p, w, h],
        out_sem.at[6],
        rs_r,
    )
    for p in range(4):
        cols = pl.ds(512 * p, 512)
        prod = dot(xa[:, pl.ds(0, 128)], wa[0, :, cols]) + dot(xa[:, pl.ds(128, 128)], wa[1, :, cols])
        part1[p] = prod.astype(BF16).reshape(8, 32, 512)
        reduce_tick(0, (p,), *args1)
    def selections(axis, main, tails):
        shape = (192, 256) if axis == 0 else (256, 192)
        d, k, r = natural(iota(shape, axis))
        q = iota(shape, 1 - axis)
        same = (d == ((q >> 3) & 7)) & (k == (q >> 6))
        r8 = q & 7
        main[...] = jnp.where(same & (r8 == r), 1.0, 0.0).astype(BF16)
        for j in range(3):
            tails[j] = jnp.where(
                same & (((r8 == 6) & (r == j)) | ((r8 == 7) & (r == j + 3))), 1.0, 0.0
            ).astype(BF16)

    def tables(g):
        quarter = iota((8, 128), 1) >> 5
        m = jnp.zeros((8, 128), F32)
        for i, slot in enumerate(GROUPS[g]):
            m = jnp.where(quarter == i, meta[slot], m)
        d, k, r = natural(iota((384, 128), 0))
        lane = iota((384, 128), 1)
        d = d.astype(F32)
        first = jnp.broadcast_to(m[0:1, :], (384, 128)) == d
        second = jnp.broadcast_to(m[1:2, :], (384, 128)) == d
        named = (first | second).astype(F32)
        ta, tb = iota((128, 128), 0), iota((128, 128), 1)
        count = dot(named.astype(BF16), ((ta < tb) & ((ta >> 5) == (tb >> 5))).astype(BF16))
        table = jnp.where((count == r.astype(F32)) & (k == (lane >> 5)), named, 0.0)
        tdisp[g] = table.astype(BF16)
        for i in range(2):
            w = jnp.where(first, m[2 + 2 * i : 3 + 2 * i, :], m[3 + 2 * i : 4 + 2 * i, :])
            tcomb[g, i] = (table * w).astype(BF16)

    meta_tick(1)
    selections(0, gm, gt)
    reduce_tick(1, range(4), *args1)
    meta_tick(2)
    tables(0)
    reduce_tick(2, range(4), *args1)
    meta_tick(3)
    selections(1, gmt, gtt)
    reduce_tick(3, range(4), *args1)
    meta_tick(4)
    local[8].wait()
    local[9].wait()
    square = jnp.zeros((32, 1), F32)
    for p in range(4):
        cols = pl.ds(512 * p, 512)
        wide = (res_ref[:, cols].astype(F32) + reduce_last(p, *args1)).astype(BF16)
        hid[:, cols] = wide
        wide = wide.astype(F32)
        square = square + jnp.sum(wide * wide, axis=1, keepdims=True)
    scale = lax.rsqrt(square * (1.0 / 2048.0) + EPS)
    gain = gain_ref[...].astype(F32)
    for i in list(range(8, 16)) + list(range(8)):
        cols = pl.ds(128 * i, 128)
        nrm[:, cols] = (hid[:, cols].astype(F32) * scale * gain[i : i + 1, :]).astype(BF16)
    for c in range(2):
        tok[c, 0] = nrm[:, pl.ds(1024 + 512 * c, 512)]

    def tok_tick(k):
        for c in range(2):
            for way in range(2):
                slots = GATHER[c][way]
                if 0 < k <= len(slots):
                    slot = k if way == 0 else 8 - k
                    received(tok.at[c, slot], tok_r.at[c, slot - 1])
                if k < len(slots):
                    to = (slots[k] + 1) % 8 if way == 0 else (slots[k] + 7) % 8
                    send(tok.at[c, slots[k]], tok.at[c, to], out_sem.at[10], tok_r.at[c, to - 1], sides[way])

    tok_tick(0)

    tail = nrm[:, pl.ds(768, 256)]
    for j in range(3):
        cols = pl.ds(256 * j, 256)
        packed = (dot(tmain[...], nrm[:, cols]) + dot(ttail[j], tail)).astype(BF16)
        outg[:, :, cols] = packed.reshape(16, 8, 256)
    for d in ORDER:
        send(outg.at[d], xbuf.at[0, d], out_sem.at[11], in_sem.at[8 + d // 8], ahead(d))
    xbuf[0, 0] = outg[0]

    def disp2(g):
        for c in range(2):
            cols = pl.ds(512 * c, 512)
            block = jnp.concatenate([tok[c, slot] for slot in GROUPS[g]], axis=0)
            out2[g, :, :, cols] = dot(tdisp[g], block).astype(BF16).reshape(16, 24, 512)
        for d in ORDER:
            send(out2.at[g, d], x2buf.at[g, d], out_sem.at[12 + g], in_sem.at[10 + 2 * g + d // 8], ahead(d))
        x2buf[g, 0] = out2[g, 0]

    def piece_at(buf, slot, piece):
        return buf.at[slot, pl.ds(4 * piece, 4)]

    def whole(pair):
        return pl.ds(8, 8) if pair else pl.ds(1, 7)

    def gather_tick(pair, k):
        if k == 0:
            received(xbuf.at[0, whole(pair)], in_sem.at[8 + pair])
        for piece in (2 * pair, 2 * pair + 1):
            for way in range(2):
                slots = GATHER[piece % 2][way]
                if 0 < k <= len(slots):
                    slot = k if way == 0 else 8 - k
                    received(piece_at(xbuf, slot, piece), ag_r.at[piece, slot - 1])
                if k < len(slots):
                    to = (slots[k] + 1) % 8 if way == 0 else (slots[k] + 7) % 8
                    send(piece_at(xbuf, slots[k], piece), piece_at(xbuf, to, piece), out_sem.at[14],
                         ag_r.at[piece, to - 1], sides[way])

    def expert(pair, g, step):
        these = pl.ds(8 * pair, 8)

        def down(cols):
            return (dot(act[0], wd[0, :, cols]) + dot(act[1], wd[1, :, cols])).astype(BF16)

        if step == 0:
            for i, slot in enumerate(GROUPS[g]):
                xcat[pl.ds(64 * i, 64), :] = xbuf[slot, these].reshape(64, 768)
            x2[:, pl.ds(0, 768)] = dot(gm[...], xcat[...]).astype(BF16)
            last = jnp.zeros((192, 256), F32)
            for j in range(3):
                last = last + dot(gt[j], xcat[:, pl.ds(256 * j, 256)])
            x2[:, pl.ds(768, 256)] = last.astype(BF16)
            received(x2buf.at[g, whole(pair)], in_sem.at[10 + 2 * g + pair])
            x2[:, pl.ds(1024, 1024)] = x2buf[g, these].reshape(192, 1024)
        if step < 2:
            gate = dot(x2[...], wg[step])
            up = dot(x2[...], wu[step])
            act[step] = (gate / (1.0 + jnp.exp(-gate)) * up).astype(BF16)
        if step == 2:
            for c in range(2):
                y2[g, these, :, pl.ds(512 * c, 512)] = down(pl.ds(1024 + 512 * c, 512)).reshape(8, 24, 512)

        if step == 3:
            last = down(pl.ds(768, 256))
            for j in range(3):
                cols = pl.ds(256 * j, 256)
                packed = (dot(gmt[...], down(cols)) + dot(gtt[j], last)).astype(BF16)
                for i, slot in enumerate(GROUPS[g]):
                    part[slot, these, :, cols] = packed[64 * i : 64 * i + 64].reshape(8, 8, 256)

    def returns(pair, g):
        for d in ORDER:
            if d // 8 == pair:
                send(y2.at[g, d], back2.at[g, d], out_sem.at[15], in_sem.at[14 + g], behind(d))
        if pair == 0:
            back2[g, 0] = y2[g, 0]

    args = (
        lambda p, s: piece_at(part, s, p),
        lambda p, w, h: rbuf.at[p, w, h],
        out_sem.at[16],
        rs_r,
    )

    def send_back(pair):
        for piece in (2 * pair, 2 * pair + 1):
            fin[pl.ds(4 * piece, 4)] = reduce_last(piece, *args).astype(BF16)
            for d in range(4 * piece, 4 * piece + 4):
                if d == 0:
                    ret[0] = fin[0]
                else:
                    send(fin.at[d], ret.at[d], out_sem.at[17], ret_r, behind(d))

    args2 = (
        lambda p, s: cpart.at[p, s],
        lambda p, w, h: rbuf2.at[p, w, h],
        out_sem.at[18],
        tok_r,
    )

    def combine(g):
        received(back2.at[g, pl.ds(1, 15)], in_sem.at[14 + g])
        for c in range(2):
            block = back2[g, :, :, pl.ds(512 * c, 512)].reshape(384, 512)
            total = dot_t(tcomb[g, 0], block) + dot_t(tcomb[g, 1], block)
            for i, slot in enumerate(GROUPS[g]):
                cpart[c, slot] = total[32 * i : 32 * i + 32].astype(BF16)

    tables(1)
    tok_tick(1)
    gather_tick(0, 0)
    tok_tick(2)
    disp2(0)
    gather_tick(1, 0)
    gather_tick(0, 1)
    tok_tick(3)
    gather_tick(0, 2)
    tok_tick(4)
    disp2(1)
    for c in local[10:]:
        c.wait()
    for c in e_duo:
        c.wait_recv()
    expert(0, 0, 0)
    gather_tick(0, 3)
    gather_tick(1, 1)
    expert(0, 0, 1)
    expert(0, 0, 2)
    expert(0, 0, 3)
    gather_tick(0, 4)
    gather_tick(1, 2)
    expert(0, 1, 0)
    expert(0, 1, 1)
    expert(0, 1, 2)
    returns(0, 1)
    expert(0, 1, 3)
    reduce_tick(0, (0, 1), *args)
    expert(1, 0, 0)
    gather_tick(1, 3)
    returns(0, 0)
    expert(1, 0, 1)
    expert(1, 0, 2)
    expert(1, 0, 3)
    gather_tick(1, 4)
    reduce_tick(1, (0, 1), *args)
    expert(1, 1, 0)
    expert(1, 1, 1)
    expert(1, 1, 2)
    returns(1, 1)
    returns(1, 0)
    expert(1, 1, 3)
    reduce_tick(0, (2, 3), *args)
    reduce_tick(2, (0, 1), *args)
    reduce_tick(1, (2, 3), *args)
    reduce_tick(3, (0, 1), *args)
    combine(1)
    reduce_tick(0, (0, 1), *args2)
    reduce_tick(2, (2, 3), *args)
    send_back(0)
    combine(0)
    reduce_tick(1, (0, 1), *args2)
    reduce_tick(3, (2, 3), *args)
    reduce_tick(2, (0, 1), *args2)
    send_back(1)
    reduce_tick(3, (0, 1), *args2)

    received(ret.at[pl.ds(1, 15)], ret_r)
    weight = [
        jnp.where(one[0], line[i : i + 1, :], 0.0) + jnp.where(one[1], line[i + 1 : i + 2, :], 0.0) for i in (2, 4)
    ]
    weight = [w.astype(BF16) for w in weight]
    last = jnp.zeros((32, 256), F32)
    for j in range(3):
        cols = pl.ds(256 * j, 256)
        block = ret[:, :, cols].reshape(128, 256)
        acc = jnp.zeros((32, 256), F32)
        for w in weight:
            acc = acc + dot_t(w * tmain[...], block)
            last = last + dot_t(w * ttail[j], block)
        out_ref[:, cols] = (hid[:, cols].astype(F32) + acc).astype(BF16)
    cols = pl.ds(768, 256)
    out_ref[:, cols] = (hid[:, cols].astype(F32) + last).astype(BF16)
    for c in range(2):
        cols = pl.ds(1024 + 512 * c, 512)
        out_ref[:, cols] = (hid[:, cols].astype(F32) + reduce_last(c, *args2)).astype(BF16)
    sent(h_in, 0)
    sent(h_docs, 1)
    for c in g_duo + [w_duo] + e_duo:
        c.wait_send()
    sent(meta.at[pl.ds(1, 7)], 4)
    sent(part1.at[:, pl.ds(1, 7)], 6)
    sent(tok.at[:, pl.ds(1, 7)], 10)
    sent(outg.at[pl.ds(1, 15)], 11)
    sent(out2.at[0, pl.ds(1, 15)], 12)
    sent(out2.at[1, pl.ds(1, 15)], 13)
    sent(xbuf.at[pl.ds(1, 7)], 14)
    sent(y2.at[:, pl.ds(1, 15)], 15)
    sent(part.at[pl.ds(1, 7)], 16)
    sent(fin.at[pl.ds(1, 15)], 17)
    sent(cpart.at[:, pl.ds(1, 7)], 18)


def shards(
    out_gate, in_gate, conv_input, conv_taps, documents, out_weight, residual, norm_gain, expert_ids, route_weights,
    gate_weight, up_weight, down_weight,
):
    hbm = pl.BlockSpec(memory_space=pl.ANY)
    dma = pltpu.SemaphoreType.DMA

    def buf(*shape, dtype=BF16):
        return pltpu.VMEM(shape, dtype)

    scratch = [
        buf(512, 128), buf(512, 128), buf(512, 128), buf(3, 128), buf(4, 128, dtype=jnp.int32), buf(32, 2048),
        buf(16, 128), buf(2, 32, dtype=jnp.int32), buf(2, 32, dtype=F32),
        buf(2, 16, 128), buf(4, 128, dtype=jnp.int32), buf(528, 128, dtype=F32), buf(528, 128, dtype=F32),
        buf(3, 256, 128), buf(256, 256), buf(2, 128, 2048), buf(4, 8, 32, 512), buf(4, 2, 4, 32, 512),
        buf(32, 2048), buf(32, 2048),
        buf(8, 32, dtype=F32), buf(8, 8, 128, dtype=F32), buf(128, 32), buf(3, 128, 32), buf(2, 384, 128),
        buf(2, 2, 384, 128), buf(192, 256), buf(3, 192, 256), buf(256, 192), buf(3, 256, 192),
        buf(2, 8, 32, 512), buf(16, 8, 768), buf(2, 16, 24, 1024), buf(8, 16, 8, 768), buf(2, 16, 24, 1024),
        buf(256, 768), buf(192, 2048), buf(2, 192, 256), buf(2, 2048, 256), buf(2, 2048, 256), buf(2, 256, 2048),
        buf(8, 16, 8, 768), buf(4, 2, 4, 4, 8, 768), buf(2, 16, 24, 1024), buf(2, 16, 24, 1024), buf(2, 8, 32, 512),
        buf(2, 2, 4, 32, 512), buf(16, 8, 768), buf(16, 8, 768),
        dma((13,)), dma((19,)), dma((16,)), dma((7,)), dma((4, 7)), dma((4, 7)), dma((2, 7)), dma,
    ]
    return pl.pallas_call(
        kernel,
        out_shape=jax.ShapeDtypeStruct((32, 2048), BF16),
        in_specs=[hbm] * 13,
        out_specs=pl.BlockSpec(memory_space=pltpu.VMEM),
        scratch_shapes=scratch,
        compiler_params=pltpu.CompilerParams(
            collective_id=0, has_side_effects=True, vmem_limit_bytes=56 * 1024 * 1024
        ),
        name="layer",
    )(
        out_gate, in_gate, conv_input, conv_taps, documents.reshape(4, 128), out_weight, residual,
        norm_gain.reshape(16, 128), expert_ids.T, route_weights.T, gate_weight, up_weight, down_weight,
    )


def solution(mesh):
    in_specs = (
        P("sp", "tp"),
        P("sp", "tp"),
        P("sp", "tp"),
        P(None, "tp"),
        P("sp"),
        P("tp", None),
        P(("sp", "tp"), None),
        P(),
        P(("sp", "tp"), None),
        P(("sp", "tp"), None),
        P("sp", None, "tp"),
        P("sp", None, "tp"),
        P("sp", "tp", None),
    )
    out_specs = P(("sp", "tp"), None)
    return jax.shard_map(shards, mesh=mesh, in_specs=in_specs, out_specs=out_specs, check_vma=False)
```

```python
import jax
import jax.numpy as jnp
from jax import lax
from jax.experimental import pallas as pl
from jax.experimental.pallas import tpu as pltpu
from jax.sharding import PartitionSpec as P

EPS = 1e-06
MESH = pl.DeviceIdType.MESH
F32 = jnp.float32
BF16 = jnp.bfloat16

GATHER = {0: ((0, 1, 2, 3), (0, 7, 6)), 1: ((0, 1, 2), (0, 7, 6, 5))}
REDUCE = {0: ((4, 5, 6, 7), (3, 2, 1)), 1: ((5, 6, 7), (4, 3, 2, 1))}
GROUPS = ((0, 1, 7, 2), (6, 3, 5, 4))
DY = (0, 2, 1, 3)
ORDER = (6, 5, 7, 4, 2, 1, 3, 10, 14, 9, 11, 13, 15, 8, 12)


def dot(a, b):
    return jnp.dot(a, b, preferred_element_type=F32)


def dot_t(a, b):
    return lax.dot_general(a, b, (((0,), (0,)), ((), ())), preferred_element_type=F32)


def iota(shape, dim):
    return lax.broadcasted_iota(jnp.int32, shape, dim)


def natural(q):
    d = (q * 2731) >> 16
    rest = q - 24 * d
    k = (rest * 10923) >> 16
    return d, k, rest - 6 * k


def kernel(
    og_hbm, ig_hbm, ci_hbm, taps_hbm, docs_hbm, ow_ref, res_hbm, gain_hbm, ids_hbm, rw_hbm, gw_ref, uw_ref, dw_ref,
    hid, out_ref,
    og_ref, ig_ref, ci_ref, taps_ref, docs_ref, res_ref, gain_ref, ids_ref, rw_ref,
    h_in, h_docs, ext, extd, gbuf, xa, wa, part1, rbuf1, nrm,
    line, meta, tmain, ttail, tdisp, tcomb, gm, gt, gmt, gtt,
    tok, outg, out2, xbuf, x2buf, xcat, x2, act, wg, wu, wd, part, rbuf, y2, back2, cpart, rbuf2, fin, ret,
    loc_sem, out_sem, in_sem, meta_r, ag_r, rs_r, tok_r, ret_r, pace_sem,
):
    sp = lax.axis_index("sp")
    tp = lax.axis_index("tp")
    core = lax.rem(tp, 2)
    z = tp // 2
    y, x = sp // 4, lax.rem(sp, 4)
    right = {"tp": lax.rem(z + 1, 8) * 2 + core}
    left = {"tp": lax.rem(z + 7, 8) * 2 + core}
    sides = (right, left)
    partner = {"tp": z * 2 + 1 - core}
    following = {"sp": lax.rem(sp + 1, 16)}

    def ahead(d):
        return {"sp": lax.rem(y + DY[d // 4], 4) * 4 + lax.rem(x + d % 4, 4)}

    def behind(d):
        return {"sp": lax.rem(y + 4 - DY[d // 4], 4) * 4 + lax.rem(x + 4 - d % 4, 4)}

    def remote(src, dst, ssem, rsem, device):
        return pltpu.make_async_remote_copy(
            src_ref=src, dst_ref=dst, send_sem=ssem, recv_sem=rsem, device_id=device, device_id_type=MESH
        )

    def send(*args):
        c = remote(*args)
        c.start()
        return c

    def sent(ref, i):
        remote(ref, ref, out_sem.at[i], in_sem.at[0], right).wait_send()

    def received(ref, sem):
        remote(ref, ref, out_sem.at[0], sem, right).wait_recv()

    barrier = pltpu.get_barrier_semaphore()
    for device in [right, left, partner]:
        pl.semaphore_signal(barrier, inc=1, device_id=device, device_id_type=MESH)
    for d in range(1, 16):
        pl.semaphore_signal(barrier, inc=1, device_id=ahead(d), device_id_type=MESH)

    def pace():
        @pl.when(core == 0)
        def _():
            pl.semaphore_signal(pace_sem, inc=1, device_id=partner, device_id_type=MESH)

        @pl.when(core == 1)
        def _():
            pl.semaphore_wait(pace_sem, 1)

    pairs = [
        (ids_hbm, ids_ref), (rw_hbm, rw_ref), (ig_hbm, ig_ref), (ci_hbm, ci_ref), (docs_hbm, docs_ref),
        (taps_hbm, taps_ref), (og_hbm, og_ref), (ow_ref, wa.at[0]), (res_hbm, res_ref), (gain_hbm, gain_ref),
        (gw_ref.at[0], wg.at[0]), (uw_ref.at[0], wu.at[0]), (dw_ref.at[0], wd.at[0]),
    ]
    local = [pltpu.make_async_copy(a, b, loc_sem.at[i]) for i, (a, b) in enumerate(pairs)]
    for c in local:
        c.start()

    local[0].wait()
    local[1].wait()
    ids = ids_ref[...]
    dy = ((ids >> 2) - y + 4) & 3
    rid = ((dy >> 1) + 2 * (dy & 1)) * 4 + (((ids & 3) - x + 4) & 3)
    weight = rw_ref[...]
    high = weight.astype(BF16).astype(F32)
    line[pl.ds(0, 2), :] = rid.astype(F32)
    line[pl.ds(2, 2), :] = high
    line[pl.ds(4, 2), :] = (weight - high).astype(BF16).astype(F32)
    line[pl.ds(6, 2), :] = jnp.zeros((2, 32), F32)
    spread = (iota((32, 128), 0) == (iota((32, 128), 1) & 31)).astype(BF16)
    meta[0] = dot(line[...].astype(BF16), spread)

    local[2].wait()
    local[3].wait()
    local[4].wait()
    local[5].wait()
    local[6].wait()
    ext[pl.ds(16, 512), :] = ig_ref[...].astype(F32) * ci_ref[...].astype(F32)
    docs = docs_ref[...].astype(F32)
    for i in range(4):
        extd[pl.ds(16 + 128 * i, 128), :] = jnp.broadcast_to(docs[i : i + 1, :], (128, 128)).T
    taps = taps_ref[...].astype(F32)

    def gated(first, count):
        pos = sp * 512 + first + iota((count, 128), 0)
        now = extd[pl.ds(16 + first, count), :]
        conv = taps[2:3, :] * ext[pl.ds(16 + first, count), :]
        for off in (1, 2):
            ok = (pos >= off) & (extd[pl.ds(16 + first - off, count), :] == now)
            earlier = taps[2 - off : 3 - off, :] * ext[pl.ds(16 + first - off, count), :]
            conv = conv + jnp.where(ok, earlier, 0.0)
        return (og_ref[pl.ds(first, count), :].astype(F32) * conv).astype(BF16)

    for j in range(1, 16):
        gbuf[j % 2, pl.ds(32 * (j // 2), 32), :] = gated(32 * j, 32)

    pl.semaphore_wait(barrier, 18)

    send(ig_ref.at[pl.ds(496, 16)], h_in.at[0], out_sem.at[0], in_sem.at[0], following)
    send(ci_ref.at[pl.ds(496, 16)], h_in.at[1], out_sem.at[0], in_sem.at[0], following)
    send(docs_ref, h_docs, out_sem.at[1], in_sem.at[1], following)
    rest = pl.ds(32, 224)
    g_duo = send(gbuf.at[1 - core, rest], gbuf.at[2, rest], out_sem.at[2], in_sem.at[2], partner)
    head = pl.ds(0, 32)

    def first_block(where):
        @pl.when(core == 1 - where)
        def _():
            send(gbuf.at[where, head], gbuf.at[2, head], out_sem.at[5], in_sem.at[4], partner)

    first_block(1)
    local[7].wait()
    w_duo = send(wa.at[0], wa.at[1], out_sem.at[3], in_sem.at[3], partner)

    e_duo = [
        send(gw_ref.at[0], wg.at[1], out_sem.at[7], in_sem.at[5], partner),
        send(uw_ref.at[0], wu.at[1], out_sem.at[8], in_sem.at[6], partner),
    ]

    def meta_tick(k):
        for way in range(2):
            slots = GATHER[0][way]
            if 0 < k <= len(slots):
                slot = k if way == 0 else 8 - k
                received(meta.at[slot], meta_r.at[slot - 1])
            if k < len(slots):
                to = (slots[k] + 1) % 8 if way == 0 else (slots[k] + 7) % 8
                send(meta.at[slots[k]], meta.at[to], out_sem.at[4], meta_r.at[to - 1], sides[way])

    meta_tick(0)
    rows = iota((128, 32), 0)
    rel, sub = rows >> 3, (rows & 7).astype(F32)
    one = [(jnp.broadcast_to(rid[k : k + 1, :], (128, 32)) == rel) for k in range(2)]
    both = (one[0] | one[1]).astype(F32)
    before = (iota((32, 32), 0) < iota((32, 32), 1)).astype(BF16)
    place = dot(both.astype(BF16), before)
    tmain[...] = (jnp.where((place == sub) & (sub < 6.0), 1.0, 0.0) * both).astype(BF16)
    for j in range(3):
        hit = ((sub == 6.0) & (place == float(j))) | ((sub == 7.0) & (place == j + 3.0))
        ttail[j] = (jnp.where(hit, 1.0, 0.0) * both).astype(BF16)

    def arrival(rsem, piece, way, hop):
        return rsem.at[piece, hop if way == 0 else len(REDUCE[piece % 2][0]) + hop]

    def reduce_hop(piece, way, hop, part_at, rbuf_at, ssem, rsem):
        slots = REDUCE[piece % 2][way]
        here = part_at(piece, slots[hop])
        if hop > 0:
            came = rbuf_at(piece, way, hop - 1)
            received(came, arrival(rsem, piece, way, hop - 1))
            here[...] = (here[...].astype(F32) + came[...].astype(F32)).astype(BF16)
        send(here, rbuf_at(piece, way, hop), ssem, arrival(rsem, piece, way, hop), sides[way])

    def reduce_tick(t, pieces, *rest):
        for piece in pieces:
            for way in range(2):
                if t < len(REDUCE[piece % 2][way]):
                    reduce_hop(piece, way, t, *rest)

    def reduce_last(piece, part_at, rbuf_at, ssem, rsem):
        total = part_at(piece, 0)[...].astype(F32)
        for way in range(2):
            hop = len(REDUCE[piece % 2][way]) - 1
            here = rbuf_at(piece, way, hop)
            received(here, arrival(rsem, piece, way, hop))
            total = total + here[...].astype(F32)
        return total

    args1 = (
        lambda p, s: part1.at[p, lax.rem(z - s + 8, 8)],
        lambda p, w, h: rbuf1.at[p, w, h],
        out_sem.at[6],
        rs_r,
    )
    def first_hop(piece, late):
        for way in range(2):
            slot = REDUCE[piece % 2][way][0]
            ready = lax.rem(z - slot + 8, 8) == 0

            @pl.when(ready if late else jnp.logical_not(ready))
            def _():
                reduce_hop(piece, way, 0, *args1)

    xa[rest, pl.ds(0, 128)] = gbuf[core, rest]
    w_duo.wait_recv()
    g_duo.wait_recv()
    xa[rest, pl.ds(128, 128)] = gbuf[2, rest]
    for p in range(4):
        cols = pl.ds(512 * p, 512)
        prod = dot(xa[rest, pl.ds(0, 128)], wa[0, :, cols]) + dot(xa[rest, pl.ds(128, 128)], wa[1, :, cols])
        part1[p, pl.ds(1, 7)] = prod.astype(BF16).reshape(7, 32, 512)
        first_hop(p, False)
    received(h_in, in_sem.at[0])
    received(h_docs, in_sem.at[1])
    ext[pl.ds(0, 16), :] = h_in[0].astype(F32) * h_in[1].astype(F32)
    old = jnp.broadcast_to(h_docs[...].astype(F32)[3:4, :], (128, 128)).T
    extd[pl.ds(0, 16), :] = old[112:128, :]
    gbuf[0, head, :] = gated(0, 32)
    first_block(0)
    e_duo.append(send(dw_ref.at[0], wd.at[1], out_sem.at[9], in_sem.at[7], partner))
    xa[head, pl.ds(0, 128)] = gbuf[core, head]
    received(gbuf.at[2, head], in_sem.at[4])
    xa[head, pl.ds(128, 128)] = gbuf[2, head]
    for p in range(4):
        cols = pl.ds(512 * p, 512)
        prod = dot(xa[head, pl.ds(0, 128)], wa[0, :, cols]) + dot(xa[head, pl.ds(128, 128)], wa[1, :, cols])
        part1[p, 0] = prod.astype(BF16)
        first_hop(p, True)

    def selections(axis, main, tails):
        shape = (192, 256) if axis == 0 else (256, 192)
        d, k, r = natural(iota(shape, axis))
        q = iota(shape, 1 - axis)
        same = (d == ((q >> 3) & 7)) & (k == (q >> 6))
        r8 = q & 7
        main[...] = jnp.where(same & (r8 == r), 1.0, 0.0).astype(BF16)
        for j in range(3):
            tails[j] = jnp.where(
                same & (((r8 == 6) & (r == j)) | ((r8 == 7) & (r == j + 3))), 1.0, 0.0
            ).astype(BF16)

    def tables(g):
        quarter = iota((8, 128), 1) >> 5
        m = jnp.zeros((8, 128), F32)
        for i, slot in enumerate(GROUPS[g]):
            m = jnp.where(quarter == i, meta[slot], m)
        d, k, r = natural(iota((384, 128), 0))
        lane = iota((384, 128), 1)
        d = d.astype(F32)
        first = jnp.broadcast_to(m[0:1, :], (384, 128)) == d
        second = jnp.broadcast_to(m[1:2, :], (384, 128)) == d
        named = (first | second).astype(F32)
        ta, tb = iota((128, 128), 0), iota((128, 128), 1)
        count = dot(named.astype(BF16), ((ta < tb) & ((ta >> 5) == (tb >> 5))).astype(BF16))
        table = jnp.where((count == r.astype(F32)) & (k == (lane >> 5)), named, 0.0)
        tdisp[g] = table.astype(BF16)
        for i in range(2):
            w = jnp.where(first, m[2 + 2 * i : 3 + 2 * i, :], m[3 + 2 * i : 4 + 2 * i, :])
            tcomb[g, i] = (table * w).astype(BF16)

    meta_tick(1)
    selections(0, gm, gt)
    reduce_tick(1, range(4), *args1)
    meta_tick(2)
    tables(0)
    pace()
    reduce_tick(2, range(4), *args1)
    meta_tick(3)
    selections(1, gmt, gtt)
    reduce_tick(3, range(4), *args1)
    meta_tick(4)
    local[8].wait()
    local[9].wait()
    square = jnp.zeros((32, 1), F32)
    for p in range(4):
        cols = pl.ds(512 * p, 512)
        wide = (res_ref[:, cols].astype(F32) + reduce_last(p, *args1)).astype(BF16)
        hid[:, cols] = wide
        wide = wide.astype(F32)
        square = square + jnp.sum(wide * wide, axis=1, keepdims=True)
    scale = lax.rsqrt(square * (1.0 / 2048.0) + EPS)
    gain = gain_ref[...].astype(F32)
    for i in list(range(8, 16)) + list(range(8)):
        cols = pl.ds(128 * i, 128)
        nrm[:, cols] = (hid[:, cols].astype(F32) * scale * gain[i : i + 1, :]).astype(BF16)
    for c in range(2):
        tok[c, 0] = nrm[:, pl.ds(1024 + 512 * c, 512)]

    def tok_tick(k):
        for c in range(2):
            for way in range(2):
                slots = GATHER[c][way]
                if 0 < k <= len(slots):
                    slot = k if way == 0 else 8 - k
                    received(tok.at[c, slot], tok_r.at[c, slot - 1])
                if k < len(slots):
                    to = (slots[k] + 1) % 8 if way == 0 else (slots[k] + 7) % 8
                    send(tok.at[c, slots[k]], tok.at[c, to], out_sem.at[10], tok_r.at[c, to - 1], sides[way])

    tok_tick(0)

    tail = nrm[:, pl.ds(768, 256)]
    for j in range(3):
        cols = pl.ds(256 * j, 256)
        packed = (dot(tmain[...], nrm[:, cols]) + dot(ttail[j], tail)).astype(BF16)
        outg[:, :, cols] = packed.reshape(16, 8, 256)
    for d in ORDER:
        send(outg.at[d], xbuf.at[0, d], out_sem.at[11], in_sem.at[8 + d // 8], ahead(d))
    xbuf[0, 0] = outg[0]

    def disp2(g):
        for c in range(2):
            cols = pl.ds(512 * c, 512)
            block = jnp.concatenate([tok[c, slot] for slot in GROUPS[g]], axis=0)
            out2[g, :, :, cols] = dot(tdisp[g], block).astype(BF16).reshape(16, 24, 512)
        for d in ORDER:
            send(out2.at[g, d], x2buf.at[g, d], out_sem.at[12 + g], in_sem.at[10 + 2 * g + d // 8], ahead(d))
        x2buf[g, 0] = out2[g, 0]

    def piece_at(buf, slot, piece):
        return buf.at[slot, pl.ds(4 * piece, 4)]

    def whole(pair):
        return pl.ds(8, 8) if pair else pl.ds(1, 7)

    def gather_tick(pair, k):
        if k == 0:
            received(xbuf.at[0, whole(pair)], in_sem.at[8 + pair])
        for piece in (2 * pair, 2 * pair + 1):
            for way in range(2):
                slots = GATHER[piece % 2][way]
                if 0 < k <= len(slots):
                    slot = k if way == 0 else 8 - k
                    received(piece_at(xbuf, slot, piece), ag_r.at[piece, slot - 1])
                if k < len(slots):
                    to = (slots[k] + 1) % 8 if way == 0 else (slots[k] + 7) % 8
                    send(piece_at(xbuf, slots[k], piece), piece_at(xbuf, to, piece), out_sem.at[14],
                         ag_r.at[piece, to - 1], sides[way])

    def expert(pair, g, step):
        these = pl.ds(8 * pair, 8)

        def down(cols):
            return (dot(act[0], wd[0, :, cols]) + dot(act[1], wd[1, :, cols])).astype(BF16)

        if step == 0:
            for i, slot in enumerate(GROUPS[g]):
                xcat[pl.ds(64 * i, 64), :] = xbuf[slot, these].reshape(64, 768)
            x2[:, pl.ds(0, 768)] = dot(gm[...], xcat[...]).astype(BF16)
            last = jnp.zeros((192, 256), F32)
            for j in range(3):
                last = last + dot(gt[j], xcat[:, pl.ds(256 * j, 256)])
            x2[:, pl.ds(768, 256)] = last.astype(BF16)
            received(x2buf.at[g, whole(pair)], in_sem.at[10 + 2 * g + pair])
            x2[:, pl.ds(1024, 1024)] = x2buf[g, these].reshape(192, 1024)
        if step < 2:
            gate = dot(x2[...], wg[step])
            up = dot(x2[...], wu[step])
            act[step] = (gate / (1.0 + jnp.exp(-gate)) * up).astype(BF16)
        if step == 2:
            for c in range(2):
                y2[g, these, :, pl.ds(512 * c, 512)] = down(pl.ds(1024 + 512 * c, 512)).reshape(8, 24, 512)

        if step == 3:
            last = down(pl.ds(768, 256))
            for j in range(3):
                cols = pl.ds(256 * j, 256)
                packed = (dot(gmt[...], down(cols)) + dot(gtt[j], last)).astype(BF16)
                for i, slot in enumerate(GROUPS[g]):
                    part[slot, these, :, cols] = packed[64 * i : 64 * i + 64].reshape(8, 8, 256)

    def returns(pair, g):
        for d in ORDER:
            if d // 8 == pair:
                send(y2.at[g, d], back2.at[g, d], out_sem.at[15], in_sem.at[14 + g], behind(d))
        if pair == 0:
            back2[g, 0] = y2[g, 0]

    args = (
        lambda p, s: piece_at(part, s, p),
        lambda p, w, h: rbuf.at[p, w, h],
        out_sem.at[16],
        rs_r,
    )

    def send_back(pair):
        for piece in (2 * pair, 2 * pair + 1):
            fin[pl.ds(4 * piece, 4)] = reduce_last(piece, *args).astype(BF16)
            for d in range(4 * piece, 4 * piece + 4):
                if d == 0:
                    ret[0] = fin[0]
                else:
                    send(fin.at[d], ret.at[d], out_sem.at[17], ret_r, behind(d))

    args2 = (
        lambda p, s: cpart.at[p, s],
        lambda p, w, h: rbuf2.at[p, w, h],
        out_sem.at[18],
        tok_r,
    )

    def combine(g):
        received(back2.at[g, pl.ds(1, 15)], in_sem.at[14 + g])
        for c in range(2):
            block = back2[g, :, :, pl.ds(512 * c, 512)].reshape(384, 512)
            total = dot_t(tcomb[g, 0], block) + dot_t(tcomb[g, 1], block)
            for i, slot in enumerate(GROUPS[g]):
                cpart[c, slot] = total[32 * i : 32 * i + 32].astype(BF16)

    tables(1)
    tok_tick(1)
    gather_tick(0, 0)
    tok_tick(2)
    disp2(0)
    gather_tick(1, 0)
    gather_tick(0, 1)
    tok_tick(3)
    gather_tick(0, 2)
    tok_tick(4)
    disp2(1)
    for c in local[10:]:
        c.wait()
    for c in e_duo:
        c.wait_recv()
    expert(0, 0, 0)
    gather_tick(0, 3)
    gather_tick(1, 1)
    expert(0, 0, 1)
    expert(0, 0, 2)
    expert(0, 0, 3)
    gather_tick(0, 4)
    gather_tick(1, 2)
    expert(0, 1, 0)
    expert(0, 1, 1)
    expert(0, 1, 2)
    returns(0, 1)
    expert(0, 1, 3)
    reduce_tick(0, (0, 1), *args)
    expert(1, 0, 0)
    gather_tick(1, 3)
    returns(0, 0)
    expert(1, 0, 1)
    expert(1, 0, 2)
    expert(1, 0, 3)
    gather_tick(1, 4)
    reduce_tick(1, (0, 1), *args)
    expert(1, 1, 0)
    expert(1, 1, 1)
    expert(1, 1, 2)
    returns(1, 1)
    returns(1, 0)
    expert(1, 1, 3)
    reduce_tick(0, (2, 3), *args)
    reduce_tick(2, (0, 1), *args)
    reduce_tick(1, (2, 3), *args)
    reduce_tick(3, (0, 1), *args)
    combine(1)
    reduce_tick(0, (0, 1), *args2)
    reduce_tick(2, (2, 3), *args)
    send_back(0)
    combine(0)
    reduce_tick(1, (0, 1), *args2)
    reduce_tick(3, (2, 3), *args)
    reduce_tick(2, (0, 1), *args2)
    send_back(1)
    reduce_tick(3, (0, 1), *args2)

    received(ret.at[pl.ds(1, 15)], ret_r)
    weight = [
        jnp.where(one[0], line[i : i + 1, :], 0.0) + jnp.where(one[1], line[i + 1 : i + 2, :], 0.0) for i in (2, 4)
    ]
    weight = [w.astype(BF16) for w in weight]
    last = jnp.zeros((32, 256), F32)
    for j in range(3):
        cols = pl.ds(256 * j, 256)
        block = ret[:, :, cols].reshape(128, 256)
        acc = jnp.zeros((32, 256), F32)
        for w in weight:
            acc = acc + dot_t(w * tmain[...], block)
            last = last + dot_t(w * ttail[j], block)
        out_ref[:, cols] = acc
    cols = pl.ds(768, 256)
    out_ref[:, cols] = last
    for c in range(2):
        cols = pl.ds(1024 + 512 * c, 512)
        out_ref[:, cols] = reduce_last(c, *args2)
    sent(h_in, 0)
    sent(h_docs, 1)
    for c in [g_duo, w_duo] + e_duo:
        c.wait_send()
    sent(gbuf.at[2, pl.ds(0, 32)], 5)
    sent(meta.at[pl.ds(1, 7)], 4)
    sent(part1.at[:, pl.ds(1, 7)], 6)
    sent(tok.at[:, pl.ds(1, 7)], 10)
    sent(outg.at[pl.ds(1, 15)], 11)
    sent(out2.at[0, pl.ds(1, 15)], 12)
    sent(out2.at[1, pl.ds(1, 15)], 13)
    sent(xbuf.at[pl.ds(1, 7)], 14)
    sent(y2.at[:, pl.ds(1, 15)], 15)
    sent(part.at[pl.ds(1, 7)], 16)
    sent(fin.at[pl.ds(1, 15)], 17)
    sent(cpart.at[:, pl.ds(1, 7)], 18)


def shards(
    out_gate, in_gate, conv_input, conv_taps, documents, out_weight, residual, norm_gain, expert_ids, route_weights,
    gate_weight, up_weight, down_weight,
):
    hbm = pl.BlockSpec(memory_space=pl.ANY)
    dma = pltpu.SemaphoreType.DMA

    def buf(*shape, dtype=BF16):
        return pltpu.VMEM(shape, dtype)

    scratch = [
        buf(512, 128), buf(512, 128), buf(512, 128), buf(3, 128), buf(4, 128, dtype=jnp.int32), buf(32, 2048),
        buf(16, 128), buf(2, 32, dtype=jnp.int32), buf(2, 32, dtype=F32),
        buf(2, 16, 128), buf(4, 128, dtype=jnp.int32), buf(528, 128, dtype=F32), buf(528, 128, dtype=F32),
        buf(3, 256, 128), buf(256, 256), buf(2, 128, 2048), buf(4, 8, 32, 512), buf(4, 2, 4, 32, 512),
        buf(32, 2048),
        buf(8, 32, dtype=F32), buf(8, 8, 128, dtype=F32), buf(128, 32), buf(3, 128, 32), buf(2, 384, 128),
        buf(2, 2, 384, 128), buf(192, 256), buf(3, 192, 256), buf(256, 192), buf(3, 256, 192),
        buf(2, 8, 32, 512), buf(16, 8, 768), buf(2, 16, 24, 1024), buf(8, 16, 8, 768), buf(2, 16, 24, 1024),
        buf(256, 768), buf(192, 2048), buf(2, 192, 256), buf(2, 2048, 256), buf(2, 2048, 256), buf(2, 256, 2048),
        buf(8, 16, 8, 768), buf(4, 2, 4, 4, 8, 768), buf(2, 16, 24, 1024), buf(2, 16, 24, 1024), buf(2, 8, 32, 512),
        buf(2, 2, 4, 32, 512), buf(16, 8, 768), buf(16, 8, 768),
        dma((13,)), dma((19,)), dma((16,)), dma((7,)), dma((4, 7)), dma((4, 7)), dma((2, 7)), dma, pltpu.SemaphoreType.REGULAR,
    ]
    hid, total = pl.pallas_call(
        kernel,
        out_shape=(pltpu.VMEM((32, 2048), BF16), pltpu.VMEM((32, 2048), F32)),
        in_specs=[hbm] * 13,
        out_specs=(pl.BlockSpec(memory_space=pltpu.VMEM),) * 2,
        scratch_shapes=scratch,
        compiler_params=pltpu.CompilerParams(
            collective_id=0, has_side_effects=True, vmem_limit_bytes=56 * 1024 * 1024
        ),
        name="layer",
    )(
        out_gate, in_gate, conv_input, conv_taps, documents.reshape(4, 128), out_weight, residual,
        norm_gain.reshape(16, 128), expert_ids.T, route_weights.T, gate_weight, up_weight, down_weight,
    )
    return (hid.astype(F32) + total).astype(BF16)


def solution(mesh):
    in_specs = (
        P("sp", "tp"),
        P("sp", "tp"),
        P("sp", "tp"),
        P(None, "tp"),
        P("sp"),
        P("tp", None),
        P(("sp", "tp"), None),
        P(),
        P(("sp", "tp"), None),
        P(("sp", "tp"), None),
        P("sp", None, "tp"),
        P("sp", None, "tp"),
        P("sp", "tp", None),
    )
    out_specs = P(("sp", "tp"), None)
    return jax.shard_map(shards, mesh=mesh, in_specs=in_specs, out_specs=out_specs, check_vma=False)
```

```python
import jax
import jax.numpy as jnp
from jax import lax
from jax.experimental import pallas as pl
from jax.experimental.pallas import tpu as pltpu
from jax.sharding import PartitionSpec as P

EPS = 1e-06
MESH = pl.DeviceIdType.MESH
F32 = jnp.float32
BF16 = jnp.bfloat16

GATHER = {0: ((0, 1, 2, 3), (0, 7, 6)), 1: ((0, 1, 2), (0, 7, 6, 5))}
REDUCE = {0: ((4, 5, 6, 7), (3, 2, 1)), 1: ((5, 6, 7), (4, 3, 2, 1))}
GROUPS = ((0, 1, 7, 2), (6, 3, 5, 4))
DY = (0, 2, 1, 3)
ORDER = (6, 5, 7, 4, 2, 1, 3, 10, 14, 9, 11, 13, 15, 8, 12)


def dot(a, b):
    return jnp.dot(a, b, preferred_element_type=F32)


def dot_t(a, b):
    return lax.dot_general(a, b, (((0,), (0,)), ((), ())), preferred_element_type=F32)


def iota(shape, dim):
    return lax.broadcasted_iota(jnp.int32, shape, dim)


def natural(q):
    d = (q * 2731) >> 16
    rest = q - 24 * d
    k = (rest * 10923) >> 16
    return d, k, rest - 6 * k


def kernel(
    og_hbm, ig_hbm, ci_hbm, taps_hbm, docs_hbm, ow_ref, res_hbm, gain_hbm, ids_hbm, rw_hbm, gw_ref, uw_ref, dw_ref,
    hid, out_ref,
    og_ref, ig_ref, ci_ref, taps_ref, docs_ref, res_ref, gain_ref, ids_ref, rw_ref,
    h_in, h_docs, ext, extd, gbuf, xa, wa, part1, rbuf1, nrm,
    line, meta, tmain, ttail, tdisp, tcomb, gm, gt, gmt, gtt,
    tok, outg, out2, xbuf, x2buf, xcat, x2, act, wg, wu, wd, part, rbuf, y2, back2, cpart, rbuf2, fin, ret,
    loc_sem, out_sem, in_sem, meta_r, ag_r, rs_r, tok_r, ret_r, pace_sem,
):
    sp = lax.axis_index("sp")
    tp = lax.axis_index("tp")
    core = lax.rem(tp, 2)
    z = tp // 2
    y, x = sp // 4, lax.rem(sp, 4)
    right = {"tp": lax.rem(z + 1, 8) * 2 + core}
    left = {"tp": lax.rem(z + 7, 8) * 2 + core}
    sides = (right, left)
    partner = {"tp": z * 2 + 1 - core}
    following = {"sp": lax.rem(sp + 1, 16)}

    def ahead(d):
        return {"sp": lax.rem(y + DY[d // 4], 4) * 4 + lax.rem(x + d % 4, 4)}

    def behind(d):
        return {"sp": lax.rem(y + 4 - DY[d // 4], 4) * 4 + lax.rem(x + 4 - d % 4, 4)}

    def remote(src, dst, ssem, rsem, device):
        return pltpu.make_async_remote_copy(
            src_ref=src, dst_ref=dst, send_sem=ssem, recv_sem=rsem, device_id=device, device_id_type=MESH
        )

    def send(*args):
        c = remote(*args)
        c.start()
        return c

    def sent(ref, i):
        remote(ref, ref, out_sem.at[i], in_sem.at[0], right).wait_send()

    def received(ref, sem):
        remote(ref, ref, out_sem.at[0], sem, right).wait_recv()

    barrier = pltpu.get_barrier_semaphore()
    for device in [right, left, partner]:
        pl.semaphore_signal(barrier, inc=1, device_id=device, device_id_type=MESH)
    for d in range(1, 16):
        pl.semaphore_signal(barrier, inc=1, device_id=ahead(d), device_id_type=MESH)

    def pace():
        @pl.when(core == 0)
        def _():
            pl.semaphore_signal(pace_sem, inc=1, device_id=partner, device_id_type=MESH)

        @pl.when(core == 1)
        def _():
            pl.semaphore_wait(pace_sem, 1)

    pairs = [
        (ids_hbm, ids_ref), (rw_hbm, rw_ref), (ig_hbm, ig_ref), (ci_hbm, ci_ref), (docs_hbm, docs_ref),
        (taps_hbm, taps_ref), (og_hbm, og_ref), (ow_ref, wa.at[0]), (res_hbm, res_ref), (gain_hbm, gain_ref),
        (gw_ref.at[0], wg.at[0]), (uw_ref.at[0], wu.at[0]), (dw_ref.at[0], wd.at[0]),
    ]
    local = [pltpu.make_async_copy(a, b, loc_sem.at[i]) for i, (a, b) in enumerate(pairs)]
    for c in local:
        c.start()

    local[0].wait()
    local[1].wait()
    ids = ids_ref[...]
    dy = ((ids >> 2) - y + 4) & 3
    rid = ((dy >> 1) + 2 * (dy & 1)) * 4 + (((ids & 3) - x + 4) & 3)
    weight = rw_ref[...]
    high = weight.astype(BF16).astype(F32)
    line[pl.ds(0, 2), :] = rid.astype(F32)
    line[pl.ds(2, 2), :] = high
    line[pl.ds(4, 2), :] = (weight - high).astype(BF16).astype(F32)
    line[pl.ds(6, 2), :] = jnp.zeros((2, 32), F32)
    spread = (iota((32, 128), 0) == (iota((32, 128), 1) & 31)).astype(BF16)
    meta[0] = dot(line[...].astype(BF16), spread)

    local[2].wait()
    local[3].wait()
    local[4].wait()
    local[5].wait()
    local[6].wait()
    ext[pl.ds(16, 512), :] = ig_ref[...].astype(F32) * ci_ref[...].astype(F32)
    docs = docs_ref[...].astype(F32)
    for i in range(4):
        extd[pl.ds(16 + 128 * i, 128), :] = jnp.broadcast_to(docs[i : i + 1, :], (128, 128)).T
    taps = taps_ref[...].astype(F32)

    def gated(first, count):
        pos = sp * 512 + first + iota((count, 128), 0)
        now = extd[pl.ds(16 + first, count), :]
        conv = taps[2:3, :] * ext[pl.ds(16 + first, count), :]
        for off in (1, 2):
            ok = (pos >= off) & (extd[pl.ds(16 + first - off, count), :] == now)
            earlier = taps[2 - off : 3 - off, :] * ext[pl.ds(16 + first - off, count), :]
            conv = conv + jnp.where(ok, earlier, 0.0)
        return (og_ref[pl.ds(first, count), :].astype(F32) * conv).astype(BF16)

    for j in range(1, 16):
        gbuf[j % 2, pl.ds(32 * (j // 2), 32), :] = gated(32 * j, 32)

    pl.semaphore_wait(barrier, 18)

    send(ig_ref.at[pl.ds(496, 16)], h_in.at[0], out_sem.at[0], in_sem.at[0], following)
    send(ci_ref.at[pl.ds(496, 16)], h_in.at[1], out_sem.at[0], in_sem.at[0], following)
    send(docs_ref, h_docs, out_sem.at[1], in_sem.at[1], following)
    rest = pl.ds(32, 224)
    g_duo = send(gbuf.at[1 - core, rest], gbuf.at[2, rest], out_sem.at[2], in_sem.at[2], partner)
    head = pl.ds(0, 32)

    def first_block(where):
        @pl.when(core == 1 - where)
        def _():
            send(gbuf.at[where, head], gbuf.at[2, head], out_sem.at[5], in_sem.at[4], partner)

    first_block(1)
    local[7].wait()
    w_duo = send(wa.at[0], wa.at[1], out_sem.at[3], in_sem.at[3], partner)

    e_duo = [
        send(gw_ref.at[0], wg.at[1], out_sem.at[7], in_sem.at[5], partner),
        send(uw_ref.at[0], wu.at[1], out_sem.at[8], in_sem.at[6], partner),
    ]

    def meta_tick(k):
        for way in range(2):
            slots = GATHER[0][way]
            if 0 < k <= len(slots):
                slot = k if way == 0 else 8 - k
                received(meta.at[slot], meta_r.at[slot - 1])
            if k < len(slots):
                to = (slots[k] + 1) % 8 if way == 0 else (slots[k] + 7) % 8
                send(meta.at[slots[k]], meta.at[to], out_sem.at[4], meta_r.at[to - 1], sides[way])

    meta_tick(0)
    rows = iota((128, 32), 0)
    rel, sub = rows >> 3, (rows & 7).astype(F32)
    one = [(jnp.broadcast_to(rid[k : k + 1, :], (128, 32)) == rel) for k in range(2)]
    both = (one[0] | one[1]).astype(F32)
    before = (iota((32, 32), 0) < iota((32, 32), 1)).astype(BF16)
    place = dot(both.astype(BF16), before)
    tmain[...] = (jnp.where((place == sub) & (sub < 6.0), 1.0, 0.0) * both).astype(BF16)
    for j in range(3):
        hit = ((sub == 6.0) & (place == float(j))) | ((sub == 7.0) & (place == j + 3.0))
        ttail[j] = (jnp.where(hit, 1.0, 0.0) * both).astype(BF16)

    def arrival(rsem, piece, way, hop):
        return rsem.at[piece, hop if way == 0 else len(REDUCE[piece % 2][0]) + hop]

    def reduce_hop(piece, way, hop, part_at, rbuf_at, ssem, rsem):
        slots = REDUCE[piece % 2][way]
        here = part_at(piece, slots[hop])
        if hop > 0:
            came = rbuf_at(piece, way, hop - 1)
            received(came, arrival(rsem, piece, way, hop - 1))
            here[...] = (here[...].astype(F32) + came[...].astype(F32)).astype(BF16)
        send(here, rbuf_at(piece, way, hop), ssem, arrival(rsem, piece, way, hop), sides[way])

    def reduce_tick(t, pieces, *rest):
        for piece in pieces:
            for way in range(2):
                if t < len(REDUCE[piece % 2][way]):
                    reduce_hop(piece, way, t, *rest)

    def reduce_last(piece, part_at, rbuf_at, ssem, rsem):
        total = part_at(piece, 0)[...].astype(F32)
        for way in range(2):
            hop = len(REDUCE[piece % 2][way]) - 1
            here = rbuf_at(piece, way, hop)
            received(here, arrival(rsem, piece, way, hop))
            total = total + here[...].astype(F32)
        return total

    args1 = (
        lambda p, s: part1.at[p, lax.rem(z - s + 8, 8)],
        lambda p, w, h: rbuf1.at[p, w, h],
        out_sem.at[6],
        rs_r,
    )
    def first_hop(piece, late):
        for way in range(2):
            slot = REDUCE[piece % 2][way][0]
            ready = lax.rem(z - slot + 8, 8) == 0

            @pl.when(ready if late else jnp.logical_not(ready))
            def _():
                reduce_hop(piece, way, 0, *args1)

    xa[rest, pl.ds(0, 128)] = gbuf[core, rest]
    w_duo.wait_recv()
    g_duo.wait_recv()
    xa[rest, pl.ds(128, 128)] = gbuf[2, rest]
    for p in range(4):
        cols = pl.ds(512 * p, 512)
        prod = dot(xa[rest, pl.ds(0, 128)], wa[0, :, cols]) + dot(xa[rest, pl.ds(128, 128)], wa[1, :, cols])
        part1[p, pl.ds(1, 7)] = prod.astype(BF16).reshape(7, 32, 512)
        first_hop(p, False)
    received(h_in, in_sem.at[0])
    received(h_docs, in_sem.at[1])
    ext[pl.ds(0, 16), :] = h_in[0].astype(F32) * h_in[1].astype(F32)
    old = jnp.broadcast_to(h_docs[...].astype(F32)[3:4, :], (128, 128)).T
    extd[pl.ds(0, 16), :] = old[112:128, :]
    gbuf[0, head, :] = gated(0, 32)
    first_block(0)
    e_duo.append(send(dw_ref.at[0], wd.at[1], out_sem.at[9], in_sem.at[7], partner))
    xa[head, pl.ds(0, 128)] = gbuf[core, head]
    received(gbuf.at[2, head], in_sem.at[4])
    xa[head, pl.ds(128, 128)] = gbuf[2, head]
    for p in range(4):
        cols = pl.ds(512 * p, 512)
        prod = dot(xa[head, pl.ds(0, 128)], wa[0, :, cols]) + dot(xa[head, pl.ds(128, 128)], wa[1, :, cols])
        part1[p, 0] = prod.astype(BF16)
        first_hop(p, True)

    def selections(axis, main, tails):
        shape = (192, 256) if axis == 0 else (256, 192)
        d, k, r = natural(iota(shape, axis))
        q = iota(shape, 1 - axis)
        same = (d == ((q >> 3) & 7)) & (k == (q >> 6))
        r8 = q & 7
        main[...] = jnp.where(same & (r8 == r), 1.0, 0.0).astype(BF16)
        for j in range(3):
            tails[j] = jnp.where(
                same & (((r8 == 6) & (r == j)) | ((r8 == 7) & (r == j + 3))), 1.0, 0.0
            ).astype(BF16)

    def tables(g):
        quarter = iota((8, 128), 1) >> 5
        m = jnp.zeros((8, 128), F32)
        for i, slot in enumerate(GROUPS[g]):
            m = jnp.where(quarter == i, meta[slot], m)
        d, k, r = natural(iota((384, 128), 0))
        lane = iota((384, 128), 1)
        d = d.astype(F32)
        first = jnp.broadcast_to(m[0:1, :], (384, 128)) == d
        second = jnp.broadcast_to(m[1:2, :], (384, 128)) == d
        named = (first | second).astype(F32)
        ta, tb = iota((128, 128), 0), iota((128, 128), 1)
        count = dot(named.astype(BF16), ((ta < tb) & ((ta >> 5) == (tb >> 5))).astype(BF16))
        table = jnp.where((count == r.astype(F32)) & (k == (lane >> 5)), named, 0.0)
        tdisp[g] = table.astype(BF16)
        for i in range(2):
            w = jnp.where(first, m[2 + 2 * i : 3 + 2 * i, :], m[3 + 2 * i : 4 + 2 * i, :])
            tcomb[g, i] = (table * w).astype(BF16)

    meta_tick(1)
    selections(0, gm, gt)
    reduce_tick(1, range(4), *args1)
    meta_tick(2)
    tables(0)
    pace()
    reduce_tick(2, range(4), *args1)
    meta_tick(3)
    selections(1, gmt, gtt)
    reduce_tick(3, range(4), *args1)
    meta_tick(4)
    local[8].wait()
    local[9].wait()
    square = jnp.zeros((32, 1), F32)
    for p in range(4):
        cols = pl.ds(512 * p, 512)
        wide = (res_ref[:, cols].astype(F32) + reduce_last(p, *args1)).astype(BF16)
        hid[:, cols] = wide
        wide = wide.astype(F32)
        square = square + jnp.sum(wide * wide, axis=1, keepdims=True)
    scale = lax.rsqrt(square * (1.0 / 2048.0) + EPS)
    gain = gain_ref[...].astype(F32)
    for i in list(range(8, 16)) + list(range(8)):
        cols = pl.ds(128 * i, 128)
        nrm[:, cols] = (hid[:, cols].astype(F32) * scale * gain[i : i + 1, :]).astype(BF16)
    for c in range(2):
        tok[c, 0] = nrm[:, pl.ds(1024 + 512 * c, 512)]

    def tok_tick(k):
        for c in range(2):
            for way in range(2):
                slots = GATHER[c][way]
                if 0 < k <= len(slots):
                    slot = k if way == 0 else 8 - k
                    received(tok.at[c, slot], tok_r.at[c, slot - 1])
                if k < len(slots):
                    to = (slots[k] + 1) % 8 if way == 0 else (slots[k] + 7) % 8
                    send(tok.at[c, slots[k]], tok.at[c, to], out_sem.at[10], tok_r.at[c, to - 1], sides[way])

    tok_tick(0)

    tail = nrm[:, pl.ds(768, 256)]
    for j in range(3):
        cols = pl.ds(256 * j, 256)
        packed = (dot(tmain[...], nrm[:, cols]) + dot(ttail[j], tail)).astype(BF16)
        outg[:, :, cols] = packed.reshape(16, 8, 256)
    for d in ORDER:
        send(outg.at[d], xbuf.at[0, d], out_sem.at[11], in_sem.at[8 + d // 8], ahead(d))
    xbuf[0, 0] = outg[0]

    def disp2(g):
        for c in range(2):
            cols = pl.ds(512 * c, 512)
            block = jnp.concatenate([tok[c, slot] for slot in GROUPS[g]], axis=0)
            out2[g, :, :, cols] = dot(tdisp[g], block).astype(BF16).reshape(16, 24, 512)
        for d in ORDER:
            send(out2.at[g, d], x2buf.at[g, d], out_sem.at[12 + g], in_sem.at[10 + 2 * g + d // 8], ahead(d))
        x2buf[g, 0] = out2[g, 0]

    def piece_at(buf, slot, piece):
        return buf.at[slot, pl.ds(4 * piece, 4)]

    def whole(pair):
        return pl.ds(8, 8) if pair else pl.ds(1, 7)

    def gather_tick(pair, k):
        if k == 0:
            received(xbuf.at[0, whole(pair)], in_sem.at[8 + pair])
        for piece in (2 * pair, 2 * pair + 1):
            for way in range(2):
                slots = GATHER[piece % 2][way]
                if 0 < k <= len(slots):
                    slot = k if way == 0 else 8 - k
                    received(piece_at(xbuf, slot, piece), ag_r.at[piece, slot - 1])
                if k < len(slots):
                    to = (slots[k] + 1) % 8 if way == 0 else (slots[k] + 7) % 8
                    send(piece_at(xbuf, slots[k], piece), piece_at(xbuf, to, piece), out_sem.at[14],
                         ag_r.at[piece, to - 1], sides[way])

    def expert(pair, g, step):
        these = pl.ds(8 * pair, 8)

        def down(cols):
            return (dot(act[0], wd[0, :, cols]) + dot(act[1], wd[1, :, cols])).astype(BF16)

        if step == 0:
            for i, slot in enumerate(GROUPS[g]):
                xcat[pl.ds(64 * i, 64), :] = xbuf[slot, these].reshape(64, 768)
            x2[:, pl.ds(0, 768)] = dot(gm[...], xcat[...]).astype(BF16)
            last = jnp.zeros((192, 256), F32)
            for j in range(3):
                last = last + dot(gt[j], xcat[:, pl.ds(256 * j, 256)])
            x2[:, pl.ds(768, 256)] = last.astype(BF16)
            received(x2buf.at[g, whole(pair)], in_sem.at[10 + 2 * g + pair])
            x2[:, pl.ds(1024, 1024)] = x2buf[g, these].reshape(192, 1024)
        if step < 2:
            gate = dot(x2[...], wg[step])
            up = dot(x2[...], wu[step])
            act[step] = (gate / (1.0 + jnp.exp(-gate)) * up).astype(BF16)
        if step == 2:
            for c in range(2):
                y2[g, these, :, pl.ds(512 * c, 512)] = down(pl.ds(1024 + 512 * c, 512)).reshape(8, 24, 512)

        if step == 3:
            last = down(pl.ds(768, 256))
            for j in range(3):
                cols = pl.ds(256 * j, 256)
                packed = (dot(gmt[...], down(cols)) + dot(gtt[j], last)).astype(BF16)
                for i, slot in enumerate(GROUPS[g]):
                    part[slot, these, :, cols] = packed[64 * i : 64 * i + 64].reshape(8, 8, 256)

    def returns(pair, g):
        for d in ORDER:
            if d // 8 == pair:
                send(y2.at[g, d], back2.at[g, d], out_sem.at[15], in_sem.at[14 + g], behind(d))
        if pair == 0:
            back2[g, 0] = y2[g, 0]

    args = (
        lambda p, s: piece_at(part, s, p),
        lambda p, w, h: rbuf.at[p, w, h],
        out_sem.at[16],
        rs_r,
    )

    def send_back(pair):
        for piece in (2 * pair, 2 * pair + 1):
            fin[pl.ds(4 * piece, 4)] = reduce_last(piece, *args).astype(BF16)
            for d in range(4 * piece, 4 * piece + 4):
                if d == 0:
                    ret[0] = fin[0]
                else:
                    send(fin.at[d], ret.at[d], out_sem.at[17], ret_r, behind(d))

    args2 = (
        lambda p, s: cpart.at[p, s],
        lambda p, w, h: rbuf2.at[p, w, h],
        out_sem.at[18],
        tok_r,
    )

    def combine(g):
        received(back2.at[g, pl.ds(1, 15)], in_sem.at[14 + g])
        for c in range(2):
            block = back2[g, :, :, pl.ds(512 * c, 512)].reshape(384, 512)
            total = dot_t(tcomb[g, 0], block) + dot_t(tcomb[g, 1], block)
            for i, slot in enumerate(GROUPS[g]):
                cpart[c, slot] = total[32 * i : 32 * i + 32].astype(BF16)

    tables(1)
    tok_tick(1)
    gather_tick(0, 0)
    tok_tick(2)
    disp2(0)
    gather_tick(1, 0)
    gather_tick(0, 1)
    tok_tick(3)
    gather_tick(0, 2)
    tok_tick(4)
    disp2(1)
    for c in local[10:]:
        c.wait()
    for c in e_duo:
        c.wait_recv()
    expert(0, 0, 0)
    gather_tick(0, 3)
    gather_tick(1, 1)
    expert(0, 0, 1)
    expert(0, 0, 2)
    expert(0, 0, 3)
    gather_tick(0, 4)
    gather_tick(1, 2)
    expert(0, 1, 0)
    expert(0, 1, 1)
    expert(0, 1, 2)
    returns(0, 1)
    expert(0, 1, 3)
    reduce_tick(0, (0, 1), *args)
    expert(1, 0, 0)
    gather_tick(1, 3)
    returns(0, 0)
    expert(1, 0, 1)
    expert(1, 0, 2)
    expert(1, 0, 3)
    reduce_tick(1, (0, 1), *args)
    gather_tick(1, 4)
    expert(1, 1, 0)
    expert(1, 1, 1)
    expert(1, 1, 2)
    returns(1, 1)
    returns(1, 0)
    expert(1, 1, 3)
    reduce_tick(0, (2, 3), *args)
    reduce_tick(2, (0, 1), *args)
    reduce_tick(1, (2, 3), *args)
    reduce_tick(3, (0, 1), *args)
    combine(1)
    reduce_tick(0, (0, 1), *args2)
    reduce_tick(2, (2, 3), *args)
    send_back(0)
    combine(0)
    reduce_tick(1, (0, 1), *args2)
    reduce_tick(3, (2, 3), *args)
    reduce_tick(2, (0, 1), *args2)
    send_back(1)
    reduce_tick(3, (0, 1), *args2)

    received(ret.at[pl.ds(1, 15)], ret_r)
    weight = [
        jnp.where(one[0], line[i : i + 1, :], 0.0) + jnp.where(one[1], line[i + 1 : i + 2, :], 0.0) for i in (2, 4)
    ]
    weight = [w.astype(BF16) for w in weight]
    last = jnp.zeros((32, 256), F32)
    for j in range(3):
        cols = pl.ds(256 * j, 256)
        block = ret[:, :, cols].reshape(128, 256)
        acc = jnp.zeros((32, 256), F32)
        for w in weight:
            acc = acc + dot_t(w * tmain[...], block)
            last = last + dot_t(w * ttail[j], block)
        out_ref[:, cols] = acc
    cols = pl.ds(768, 256)
    out_ref[:, cols] = last
    for c in range(2):
        cols = pl.ds(1024 + 512 * c, 512)
        out_ref[:, cols] = reduce_last(c, *args2)
    sent(h_in, 0)
    sent(h_docs, 1)
    for c in [g_duo, w_duo] + e_duo:
        c.wait_send()
    sent(gbuf.at[2, pl.ds(0, 32)], 5)
    sent(meta.at[pl.ds(1, 7)], 4)
    sent(part1.at[:, pl.ds(1, 7)], 6)
    sent(tok.at[:, pl.ds(1, 7)], 10)
    sent(outg.at[pl.ds(1, 15)], 11)
    sent(out2.at[0, pl.ds(1, 15)], 12)
    sent(out2.at[1, pl.ds(1, 15)], 13)
    sent(xbuf.at[pl.ds(1, 7)], 14)
    sent(y2.at[:, pl.ds(1, 15)], 15)
    sent(part.at[pl.ds(1, 7)], 16)
    sent(fin.at[pl.ds(1, 15)], 17)
    sent(cpart.at[:, pl.ds(1, 7)], 18)


def shards(
    out_gate, in_gate, conv_input, conv_taps, documents, out_weight, residual, norm_gain, expert_ids, route_weights,
    gate_weight, up_weight, down_weight,
):
    hbm = pl.BlockSpec(memory_space=pl.ANY)
    dma = pltpu.SemaphoreType.DMA

    def buf(*shape, dtype=BF16):
        return pltpu.VMEM(shape, dtype)

    scratch = [
        buf(512, 128), buf(512, 128), buf(512, 128), buf(3, 128), buf(4, 128, dtype=jnp.int32), buf(32, 2048),
        buf(16, 128), buf(2, 32, dtype=jnp.int32), buf(2, 32, dtype=F32),
        buf(2, 16, 128), buf(4, 128, dtype=jnp.int32), buf(528, 128, dtype=F32), buf(528, 128, dtype=F32),
        buf(3, 256, 128), buf(256, 256), buf(2, 128, 2048), buf(4, 8, 32, 512), buf(4, 2, 4, 32, 512),
        buf(32, 2048),
        buf(8, 32, dtype=F32), buf(8, 8, 128, dtype=F32), buf(128, 32), buf(3, 128, 32), buf(2, 384, 128),
        buf(2, 2, 384, 128), buf(192, 256), buf(3, 192, 256), buf(256, 192), buf(3, 256, 192),
        buf(2, 8, 32, 512), buf(16, 8, 768), buf(2, 16, 24, 1024), buf(8, 16, 8, 768), buf(2, 16, 24, 1024),
        buf(256, 768), buf(192, 2048), buf(2, 192, 256), buf(2, 2048, 256), buf(2, 2048, 256), buf(2, 256, 2048),
        buf(8, 16, 8, 768), buf(4, 2, 4, 4, 8, 768), buf(2, 16, 24, 1024), buf(2, 16, 24, 1024), buf(2, 8, 32, 512),
        buf(2, 2, 4, 32, 512), buf(16, 8, 768), buf(16, 8, 768),
        dma((13,)), dma((19,)), dma((16,)), dma((7,)), dma((4, 7)), dma((4, 7)), dma((2, 7)), dma, pltpu.SemaphoreType.REGULAR,
    ]
    hid, total = pl.pallas_call(
        kernel,
        out_shape=(pltpu.VMEM((32, 2048), BF16), pltpu.VMEM((32, 2048), F32)),
        in_specs=[hbm] * 13,
        out_specs=(pl.BlockSpec(memory_space=pltpu.VMEM),) * 2,
        scratch_shapes=scratch,
        compiler_params=pltpu.CompilerParams(
            collective_id=0, has_side_effects=True, vmem_limit_bytes=56 * 1024 * 1024
        ),
        name="layer",
    )(
        out_gate, in_gate, conv_input, conv_taps, documents.reshape(4, 128), out_weight, residual,
        norm_gain.reshape(16, 128), expert_ids.T, route_weights.T, gate_weight, up_weight, down_weight,
    )
    return (hid.astype(F32) + total).astype(BF16)


def solution(mesh):
    in_specs = (
        P("sp", "tp"),
        P("sp", "tp"),
        P("sp", "tp"),
        P(None, "tp"),
        P("sp"),
        P("tp", None),
        P(("sp", "tp"), None),
        P(),
        P(("sp", "tp"), None),
        P(("sp", "tp"), None),
        P("sp", None, "tp"),
        P("sp", None, "tp"),
        P("sp", "tp", None),
    )
    out_specs = P(("sp", "tp"), None)
    return jax.shard_map(shards, mesh=mesh, in_specs=in_specs, out_specs=out_specs, check_vma=False)
```
